32 devices in a mesh: ep: 16 (over z, y, core), tp: 2 (over x).
Axes of the slice: x: 2, y: 2, z: 4, core: 2. Of those that a mesh axis runs over, the one named last changes fastest.
Arguments:
- tokens: bfloat16 [2048, 2048], P('ep'), may hold values from -6 to 6
- expert_ids: int32 [2048, 2], P('ep'), may hold values from 0 to 15, as said below
- route_weights: bfloat16 [2048, 2], P('ep'), may hold values from 0.099609375 to 1
- cotangent: bfloat16 [2048, 2048], P('ep'), may hold values from -3 to 3
- w_gate: bfloat16 [16, 2048, 512], P('ep', None, 'tp'), may hold values from -0.125 to 0.125
- w_up: bfloat16 [16, 2048, 512], P('ep', None, 'tp'), may hold values from -0.125 to 0.125
- w_down: bfloat16 [16, 512, 2048], P('ep', 'tp'), may hold values from -0.25 to 0.25
Outputs:
- token_grad: bfloat16 [2048, 2048], P('ep', 'tp')
- route_grad: bfloat16 [2048, 2], P('ep')
- grad_gate: bfloat16 [16, 2048, 512], P('ep', None, 'tp')
- grad_up: bfloat16 [16, 2048, 512], P('ep', None, 'tp')
- grad_down: bfloat16 [16, 512, 2048], P('ep', 'tp')
- gate_rows: float32 [16, 2048], P('ep')
- up_rows: float32 [16, 2048], P('ep')
- down_rows: float32 [16, 512], P('ep', 'tp')
The draws below stay inside these ranges and needn't reach their ends.
Inputs may be any that keep to these rules, and one draw needn't show every extreme that they name: `expert_ids`: each row names 2 different experts of one group: both lie in g * 4 to (g + 1) * 4 - 1 for the row's group g. In the rows of one device (aligned blocks of 128 rows) no expert is named more than 32 times, and in every block some expert is named exactly 32 times.
All inputs are finite; a program needn't handle non-finite values.
Results may differ from the reference program's by a relative error of at most 0.012.
Values may be sent and summed in bfloat16 or wider, within the bound.
A program may use at most 64 MiB of HBM per device.

```python
import jax
import jax.numpy as jnp
from jax import lax

D = 2048
F = 512
GROUPS = 4
TOPK = 2
TOK_DEV = 128
EXPERTS = 16
CAP = 32
TOKENS = 2048
N_EP = 16
N_TP = 2


def draw_expert_ids(key, part):
    per_group = EXPERTS // GROUPS
    blocks = TOKENS // TOK_DEV
    hot_group = jax.random.randint(jax.random.fold_in(key, 11), (), 0, GROUPS)
    hot_member = jax.random.randint(jax.random.fold_in(key, 12), (), 0, per_group)
    block_keys = jax.random.split(jax.random.fold_in(key, 13), blocks)
    group_ids = jnp.arange(GROUPS, dtype=jnp.int32)
    member_ids = jnp.arange(per_group, dtype=jnp.int32)

    def one_block(block_key):
        key_a, key_b, key_c, key_d, key_e = jax.random.split(block_key, 5)
        hot_size = jax.random.randint(key_a, (), max(CAP, TOK_DEV // 4), TOK_DEV // 2 + 1)
        remain = TOK_DEV - hot_size
        third = remain // 3
        jitter = remain // 8
        first_size = jax.random.randint(key_b, (), third - jitter, third + jitter + 1)
        second_size = jax.random.randint(key_c, (), third - jitter, third + jitter + 1)
        others = jnp.stack([first_size, second_size, remain - first_size - second_size])
        other_slot = jnp.minimum((group_ids - hot_group - 1) % GROUPS, 2)
        sizes = jnp.where(group_ids == hot_group, hot_size, others[other_slot]).astype(jnp.int32)
        ends = jnp.cumsum(sizes)
        starts = ends - sizes
        fill_step = jnp.maximum(jnp.minimum(CAP, sizes), 1)
        ranks = jax.random.permutation(key_d, TOK_DEV).astype(jnp.int32)
        member_group = jnp.sum((ranks[:, None] >= ends[None, :]).astype(jnp.int32), axis=1)
        inner = ranks - starts[member_group]
        count = sizes[member_group]
        stride = fill_step[member_group]
        scores = jax.random.randint(key_e, (GROUPS, per_group), 0, 1 << 20) * per_group + member_ids[None, :]
        pinned = (group_ids[:, None] == hot_group) & (member_ids[None, :] == hot_member)
        scores = jnp.where(pinned, -1, scores)
        ordering = jnp.argsort(scores, axis=1).astype(jnp.int32)
        first_pick = ordering[member_group, inner // stride]
        second_pick = ordering[member_group, (inner + count) // stride]
        base_ids = member_group * per_group
        return jnp.stack([base_ids + first_pick, base_ids + second_pick], axis=1)
    return jax.vmap(one_block)(block_keys).reshape(TOKENS, TOPK).astype(jnp.int32)


def block_levels(key, extent, pieces, least, largest):
    loudness = 1.0
    for position, parts in pieces:
        steps = jax.random.uniform(jax.random.fold_in(jax.random.fold_in(key, 6), position), (parts,), jnp.float32, least / len(pieces), largest / len(pieces))
        loudness = loudness * jnp.repeat(jnp.exp(steps), extent[position] // parts).reshape((-1,) + (1,) * (len(extent) - 1 - position))
    return loudness


def noise(rng, shape, spread, bound, cuts=(), kind=jnp.bfloat16):
    result = jax.random.normal(rng, shape, jnp.float32) * spread
    if len(cuts) > 0:
        result = block_levels(rng, shape, cuts, -0.22, 0.18) * result
    return jnp.clip(result, min=-bound, max=bound).astype(kind)


def setup_inputs(seed: int = 0) -> dict:
    streams_of = jax.random.split(jax.random.key(seed), 8)
    tokens = noise(streams_of[0], (TOKENS, D), 1.0, 6.0, ((0, 16),))
    expert_ids = draw_expert_ids(jax.random.fold_in(streams_of[7], 71), 0)
    route_weights = jnp.clip(0.099609375 + 0.9003906 * jax.random.uniform(streams_of[2], (TOKENS, TOPK), jnp.float32) ** block_levels(streams_of[2], (TOKENS, TOPK), ((0, 16),), -0.2, 0.2), 0.099609375, 1.0).astype(jnp.bfloat16)
    cotangent = noise(streams_of[3], (TOKENS, D), 0.5, 3.0, ((0, 16),))
    w_gate = noise(streams_of[4], (EXPERTS, D, F), D ** -0.5, 0.125, ((0, 16), (2, 2)))
    w_up = noise(streams_of[5], (EXPERTS, D, F), D ** -0.5, 0.125, ((0, 16), (2, 2)))
    w_down = noise(streams_of[6], (EXPERTS, F, D), F ** -0.5, 0.25, ((0, 16), (1, 2)))
    return {"tokens": tokens, "expert_ids": expert_ids, "route_weights": route_weights, "cotangent": cotangent, "w_gate": w_gate, "w_up": w_up, "w_down": w_down}


def reference(tokens, expert_ids, route_weights, cotangent, w_gate, w_up, w_down):
    assigns = TOKENS * TOPK
    slot_total = N_EP * CAP
    quarter = F // N_TP
    flat_ids = expert_ids.reshape(-1).astype(jnp.int32)
    weight_flat = jnp.concatenate([route_weights.reshape(-1).astype(jnp.float32), jnp.zeros((1,), jnp.float32)])
    rows_pad = jnp.concatenate([tokens, jnp.zeros((1, D), jnp.bfloat16)], axis=0)
    cot_pad = jnp.concatenate([cotangent, jnp.zeros((1, D), jnp.bfloat16)], axis=0)

    def per_expert(expert):
        picked = jnp.nonzero(flat_ids == expert, size=slot_total, fill_value=assigns)[0].astype(jnp.int32)
        holder = (picked // TOPK).astype(jnp.int32)
        slot_rows = rows_pad[holder]
        slot_cot = cot_pad[holder]
        slot_scale = weight_flat[picked]
        gate_cols = w_gate[expert]
        up_cols = w_up[expert]
        down_rows_w = w_down[expert]
        gate_pre = jnp.dot(slot_rows, gate_cols, preferred_element_type=jnp.float32)
        up_pre = jnp.dot(slot_rows, up_cols, preferred_element_type=jnp.float32)
        hidden_back = lax.dot_general(slot_cot, down_rows_w, (((1,), (1,)), ((), ())), preferred_element_type=jnp.float32)
        gate_sig = jax.nn.sigmoid(gate_pre)
        activated = gate_pre * gate_sig
        hidden = activated * up_pre
        route_sum = jnp.sum(hidden * hidden_back, axis=1)
        hidden_cot = slot_scale[:, None] * hidden_back
        up_cot = (hidden_cot * activated).astype(jnp.bfloat16)
        gate_cot = (hidden_cot * up_pre * gate_sig * (1.0 + gate_pre * (1.0 - gate_sig))).astype(jnp.bfloat16)
        weighted_hidden = (slot_scale[:, None] * hidden).astype(jnp.bfloat16)
        grad_down_e = lax.dot_general(weighted_hidden, slot_cot, (((0,), (0,)), ((), ())), preferred_element_type=jnp.float32).astype(jnp.bfloat16)
        grad_gate_e = lax.dot_general(slot_rows, gate_cot, (((0,), (0,)), ((), ())), preferred_element_type=jnp.float32).astype(jnp.bfloat16)
        grad_up_e = lax.dot_general(slot_rows, up_cot, (((0,), (0,)), ((), ())), preferred_element_type=jnp.float32).astype(jnp.bfloat16)
        gate_blocks = gate_cot.astype(jnp.float32).reshape(slot_total, N_TP, quarter)
        up_blocks = up_cot.astype(jnp.float32).reshape(slot_total, N_TP, quarter)
        gate_w_blocks = gate_cols.astype(jnp.float32).reshape(D, N_TP, quarter)
        up_w_blocks = up_cols.astype(jnp.float32).reshape(D, N_TP, quarter)
        block_part = jnp.einsum('sjf,djf->sjd', gate_blocks, gate_w_blocks, precision=lax.Precision.HIGHEST)
        block_part = block_part + jnp.einsum('sjf,djf->sjd', up_blocks, up_w_blocks, precision=lax.Precision.HIGHEST)
        block_round = lax.optimization_barrier(block_part.astype(jnp.bfloat16))
        pair_grad = jnp.sum(block_round.astype(jnp.float32), axis=1).astype(jnp.bfloat16)
        return grad_gate_e, grad_up_e, grad_down_e, pair_grad, route_sum.astype(jnp.bfloat16), picked

    grad_gate, grad_up, grad_down, pair_grad, route_part, picked = lax.map(per_expert, jnp.arange(EXPERTS, dtype=jnp.int32))
    index_all = picked.reshape(-1)
    token_acc = jnp.zeros((assigns + 1, D), jnp.float32).at[index_all].set(pair_grad.reshape(-1, D).astype(jnp.float32))
    token_grad = jnp.sum(token_acc[:assigns].reshape(TOKENS, TOPK, D), axis=1).astype(jnp.bfloat16)
    route_acc = jnp.zeros((assigns + 1,), jnp.bfloat16).at[index_all].set(route_part.reshape(-1))
    route_grad = route_acc[:assigns].reshape(TOKENS, TOPK)
    gate_rows = jnp.sum(jnp.square(grad_gate.astype(jnp.float32)), axis=2)
    up_rows = jnp.sum(jnp.square(grad_up.astype(jnp.float32)), axis=2)
    down_rows = jnp.sum(jnp.square(grad_down.astype(jnp.float32)), axis=2)
    return (token_grad, route_grad, grad_gate, grad_up, grad_down, gate_rows, up_rows, down_rows)
```

```python
import functools

import jax
import jax.numpy as jnp
from jax import lax
from jax.experimental import pallas as pl
from jax.experimental.layout import Layout, with_layout_constraint
from jax.experimental.pallas import tpu as pltpu
from jax.sharding import PartitionSpec as P

MESH = pl.DeviceIdType.MESH
LANES = 128
TILE = 256
SHARED = (0, 4, 2, 2)
GROUPS = 4


def greet(experts, splits, me, col):
    barrier = pltpu.get_barrier_semaphore()

    @pl.loop(1, experts)
    def _(off):
        pl.semaphore_signal(
            barrier, inc=1, device_id={"ep": lax.rem(me + off, experts), "tp": col}, device_id_type=MESH
        )

    for shift in range(1, splits):
        pl.semaphore_signal(
            barrier, inc=1, device_id={"ep": me, "tp": lax.rem(col + shift, splits)}, device_id_type=MESH
        )
    return barrier


def remote(src, dst, send, recv, ep, tp):
    return pltpu.make_async_remote_copy(
        src_ref=src,
        dst_ref=dst,
        send_sem=send,
        recv_sem=recv,
        device_id={"ep": ep, "tp": tp},
        device_id_type=MESH,
    )


def partner(group, step):
    if step == 0:
        return group
    if step == 1:
        return group + 1 - 2 * lax.rem(group, 2)
    if step == 2:
        return lax.rem(group + 2, GROUPS)
    return GROUPS - 1 - group


def column_plan(model_width, splits):
    plan = []
    for eighths in SHARED:
        shared = model_width * eighths // 8 // (splits * LANES) * (splits * LANES) if splits == 2 else 0
        cut = (model_width - shared) // splits
        plan.append((cut, cut + shared))
    return plan


def layer_kernel(
    experts, splits,
    tokens_ref, cot_ref, gsel_ref, choice_ref, scale_ref, gate_hbm, up_hbm, down_hbm,
    token_out, back_route, gate_out, up_out, square_out, down_out, down_square_out,
    packed, landed, landed_choice, stage, rows, scale_in, wide, down, cots, weighted,
    part, peer_part, total, gathered, finished, back, route_mine, peer_route, route_total,
    square_mine, peer_square, down_acc,
    far_send, far_recv, near_send, near_recv, relay_send, relay_recv, scale_send, scale_recv,
    swap_send, swap_recv, join_send, join_recv, home_send, home_recv, small_send, small_recv,
    route_send, route_recv, square_send, square_recv, local,
):
    me = lax.axis_index("ep")
    col = lax.axis_index("tp")
    members = experts // GROUPS
    group = me // members
    seat = lax.rem(me, members)
    model_width = tokens_ref.shape[1]
    capacity = rows.shape[3]
    span = members * capacity
    hidden_width = down.shape[0]
    width = model_width // splits
    f32, bf16 = jnp.float32, jnp.bfloat16
    plan = column_plan(model_width, splits)
    places = [partner(group, step) for step in range(GROUPS)]
    barrier = greet(experts, splits, me, col)
    inputs = (tokens_ref, cot_ref)

    weight_loads = (
        pltpu.make_async_copy(gate_hbm, wide.at[:, pl.ds(0, hidden_width)], local.at[0]),
        pltpu.make_async_copy(up_hbm, wide.at[:, pl.ds(hidden_width, hidden_width)], local.at[1]),
        pltpu.make_async_copy(down_hbm, down, local.at[2]),
    )
    for load in weight_loads:
        load.start()

    def window(step):
        cut, wide_cut = plan[step]
        return pl.ds(pl.multiple_of(col * cut, LANES), wide_cut)

    def relay_part(step, which):
        cut, wide_cut = plan[step]
        return pl.ds(pl.multiple_of(which * wide_cut, LANES), cut)

    def around(hop):
        return lax.rem(seat + hop, members)

    def before(hop):
        return lax.rem(seat + members - hop, members)

    def far_copy(step, i):
        if i == 2:
            source, target = choice_ref.at[places[step]], landed_choice.at[step]
        else:
            cols = pl.ds(0, plan[step][1])
            source, target = packed.at[i, step, :, cols], landed.at[i, step, :, cols]
        return remote(
            source, target, far_send.at[i, step], far_recv.at[i, step],
            places[step] * members + seat, col,
        )

    def scale_copy(step, hop):
        there = places[step] * members + around(hop)
        return remote(
            scale_ref.at[there], scale_in.at[step, seat],
            scale_send.at[step, hop], scale_recv.at[step, hop], there, col,
        )

    def near_copy(step, hop, i):
        if step == 0:
            source = stage.at[i, 0, around(hop), :, window(0)]
        else:
            source = stage.at[i, step, around(hop), :, pl.ds(0, plan[step][1])]
        return remote(
            source, rows.at[i, step, seat, :, window(step)],
            near_send.at[i, step, hop], near_recv.at[i, step, hop], group * members + around(hop), col,
        )

    def relay(step, hop, shift, i, which):
        block = rows.at[i, step, before(hop), :, relay_part(step, which)]
        return remote(
            block, block, relay_send.at[i, shift - 1, step, hop], relay_recv.at[i, shift - 1, step, hop],
            me, lax.rem(col + shift, splits),
        )

    def swap(step, hop, shift):
        peer = lax.rem(col + shift, splits)
        theirs = pl.ds(pl.multiple_of(peer * width, LANES), width)
        return remote(
            part.at[step, around(hop), :, theirs], peer_part.at[shift - 1, step, around(hop)],
            swap_send.at[shift - 1, step, hop], swap_recv.at[shift - 1, step, hop], me, peer,
        )

    def small_route(step, shift):
        return remote(
            route_mine.at[step], peer_route.at[shift - 1, step],
            small_send.at[shift - 1, step], small_recv.at[shift - 1, step],
            me, lax.rem(col + shift, splits),
        )

    def small_square(shift):
        return remote(
            square_mine, peer_square.at[shift - 1], square_send.at[shift - 1], square_recv.at[shift - 1],
            me, lax.rem(col + shift, splits),
        )

    def join_copy(step, hop):
        return remote(
            total.at[step, hop], gathered.at[step, seat],
            join_send.at[step, hop], join_recv.at[step, hop], group * members + around(hop), col,
        )

    def home_copy(step):
        return remote(
            finished.at[step], back.at[group], home_send.at[step], home_recv.at[step],
            places[step] * members + seat, col,
        )

    def route_copy(step, hop):
        there = places[step] * members + around(hop)
        return remote(
            route_total.at[step], back_route.at[me], route_send.at[step, hop], route_recv.at[step, hop],
            there, col,
        )

    def pack(step, i):
        source = inputs[i][:, window(step)] if step else inputs[i][...]
        return jnp.dot(gsel_ref[places[step]], source, preferred_element_type=f32).astype(bf16)

    def spread(step, i, block):
        choice = landed_choice[step] if step else choice_ref[group]
        value = lax.dot_general(choice, block, (((0,), (0,)), ((), ())), preferred_element_type=f32)
        wide_cut = block.shape[1]
        stage[i, step, :, :, pl.ds(0, wide_cut)] = value.astype(bf16).reshape(members, capacity, wide_cut)

        @pl.loop(1, members)
        def _(hop):
            near_copy(step, hop, i).start()

        cols = window(step) if step else pl.ds(0, wide_cut)
        rows[i, step, seat, :, cols] = stage[i, step, seat, :, pl.ds(0, wide_cut)]
        if step:
            for shift in range(1, splits):
                relay(step, 0, shift, i, col).start()

    def arrive(step, i):
        if i == 0:
            far_copy(step, 2).wait_recv()
        far_copy(step, i).wait_recv()
        spread(step, i, landed[i, step, :, pl.ds(0, plan[step][1])])

    def forward(step, i):
        @pl.loop(1, members)
        def _(hop):
            near_copy(step, hop, i).wait_recv()
            for shift in range(1, splits):
                relay(step, hop, shift, i, col).start()

    def complete(step):
        @pl.loop(0 if step else 1, members)
        def _(hop):
            for shift in range(1, splits):
                for i in range(2):
                    relay(step, hop, shift, i, lax.rem(col + splits - shift, splits)).wait_recv()

        @pl.loop(0 if step else 1, members)
        def _(hop):
            scale_copy(step, hop).wait_recv()

    def compute(step):
        slot_rows = rows[0, step].reshape(span, model_width)
        slot_cot = rows[1, step].reshape(span, model_width)
        pre = jnp.dot(slot_rows, wide[...], preferred_element_type=f32)
        gate_pre, up_pre = pre[:, :hidden_width], pre[:, hidden_width:]
        hidden_back = lax.dot_general(
            slot_cot, down[...], (((1,), (1,)), ((), ())), preferred_element_type=f32
        )
        spread_scale = jnp.broadcast_to(scale_in[step], (members, capacity, LANES))
        lane = lax.broadcasted_iota(jnp.int32, (members, capacity, LANES), 2)
        slot = lax.broadcasted_iota(jnp.int32, (members, capacity, LANES), 1)
        scale = jnp.sum(jnp.where(lane == slot, spread_scale, 0.0), axis=2, keepdims=True)
        scale = scale.reshape(span, 1)
        gate_sig = jax.nn.sigmoid(gate_pre)
        activated = gate_pre * gate_sig
        hidden = activated * up_pre
        route = hidden * hidden_back
        folded = route[:, :LANES]
        for start in range(LANES, hidden_width, LANES):
            folded = folded + route[:, start : start + LANES]
        route_mine[step] = jnp.sum(folded.T, axis=0, keepdims=True)
        hidden_cot = scale * hidden_back
        up_cot = (hidden_cot * activated).astype(bf16)
        gate_cot = (hidden_cot * up_pre * gate_sig * (1.0 + gate_pre * (1.0 - gate_sig))).astype(bf16)
        slots = pl.ds(step * span, span)
        cots[slots, pl.ds(0, hidden_width)] = gate_cot
        cots[slots, pl.ds(hidden_width, hidden_width)] = up_cot
        weighted[slots, :] = (scale * hidden).astype(bf16)
        both = cots[slots, :]

        @pl.loop(0, model_width // (2 * TILE))
        def _(tile):
            cols = pl.ds(pl.multiple_of(tile * 2 * TILE, LANES), 2 * TILE)
            term = lax.dot_general(
                both, wide[cols, :], (((1,), (1,)), ((), ())), preferred_element_type=f32
            )
            part[step, :, :, cols] = term.astype(bf16).reshape(members, capacity, 2 * TILE)

        for shift in range(1, splits):
            small_route(step, shift).start()

    def send_swaps(step):
        @pl.loop(1, members + 1)
        def _(turn):
            for shift in range(1, splits):
                swap(step, lax.rem(turn, members), shift).start()

    def route_home(step):
        value = route_mine[step]
        for shift in range(1, splits):
            small_route(step, shift).wait_recv()
            value = value + peer_route[shift - 1, step]
        route_total[step] = value
        if step == 0:
            back_route[me] = value

        @pl.loop(0 if step else 1, members)
        def _(hop):
            route_copy(step, hop).start()

    def block_total(step, hop):
        source = around(hop)
        for shift in range(1, splits):
            swap(step, hop, shift).wait_recv()
        mine = pl.ds(pl.multiple_of(col * width, LANES), width)
        value = part[step, source, :, mine].astype(f32)
        for shift in range(1, splits):
            value = value + peer_part[shift - 1, step, source].astype(f32)
        return value.astype(bf16)

    def reduce(step):
        @pl.loop(1, members)
        def _(hop):
            total[step, hop] = block_total(step, hop)
            join_copy(step, hop).start()

        gathered[step, seat] = block_total(step, 0)

    def collect(step):
        @pl.loop(1, members)
        def _(hop):
            join_copy(step, hop).wait_recv()

        pairs = gathered[step].reshape(span, width)
        choice = landed_choice[step] if step else choice_ref[group]
        summed = jnp.dot(choice, pairs, preferred_element_type=f32).astype(bf16)
        if step:
            finished[step] = summed
            home_copy(step).start()
        else:
            back[group] = summed

    def lane_sums(value):
        folded = value[:, :LANES]
        for start in range(LANES, value.shape[1], LANES):
            folded = folded + value[:, start : start + LANES]
        return folded

    def grads_in():
        @pl.loop(0, model_width // TILE)
        def _(tile):
            cols = pl.ds(pl.multiple_of(tile * TILE, LANES), TILE)
            left = rows[0, :, :, :, cols].reshape(GROUPS * span, TILE)
            grad = lax.dot_general(
                left, cots[...], (((0,), (0,)), ((), ())), preferred_element_type=f32
            ).astype(bf16)
            for n, out in enumerate((gate_out, up_out)):
                value = grad[:, n * hidden_width : (n + 1) * hidden_width]
                out[cols, :] = value
                square = lane_sums(jnp.square(value.astype(f32)))
                square_mine[n, :, cols] = jnp.sum(square.T, axis=0, keepdims=True)

        for shift in range(1, splits):
            small_square(shift).start()

    def grads_down():
        down_acc[...] = jnp.zeros_like(down_acc)

        @pl.loop(0, model_width // (2 * TILE))
        def _(tile):
            cols = pl.ds(pl.multiple_of(tile * 2 * TILE, LANES), 2 * TILE)
            right = rows[1, :, :, :, cols].reshape(GROUPS * span, 2 * TILE)
            grad = lax.dot_general(
                weighted[...], right, (((0,), (0,)), ((), ())), preferred_element_type=f32
            ).astype(bf16)
            down_out[:, cols] = grad
            down_acc[...] += lane_sums(jnp.square(grad.astype(f32)))

        down_square_out[...] = jnp.sum(down_acc[...].T, axis=0, keepdims=True)

    packed[0, 1, :, pl.ds(0, plan[1][1])] = pack(1, 0)
    packed[1, 1, :, pl.ds(0, plan[1][1])] = pack(1, 1)
    pl.semaphore_wait(barrier, experts - 1 + splits - 1)
    for i in (2, 0, 1):
        far_copy(1, i).start()
    for step in range(2, GROUPS):
        far_copy(step, 2).start()
        for i in range(2):
            packed[i, step, :, pl.ds(0, plan[step][1])] = pack(step, i)
            far_copy(step, i).start()
    for i in range(2):
        spread(0, i, pack(0, i))
    scale_in[0, seat] = scale_ref[me]
    for step in range(GROUPS):

        @pl.loop(0 if step else 1, members)
        def _(hop):
            scale_copy(step, hop).start()

    forward(0, 0)
    arrive(1, 0)
    forward(0, 1)
    arrive(1, 1)
    forward(1, 0)
    for load in weight_loads:
        load.wait()
    complete(0)
    compute(0)
    arrive(2, 0)
    forward(1, 1)
    arrive(2, 1)
    forward(2, 0)
    complete(1)
    compute(1)
    send_swaps(1)
    arrive(3, 0)
    forward(2, 1)
    arrive(3, 1)
    forward(3, 0)
    complete(2)
    compute(2)
    send_swaps(2)
    forward(3, 1)
    route_home(0)
    route_home(1)
    reduce(1)
    complete(3)
    compute(3)
    send_swaps(3)
    send_swaps(0)
    collect(1)
    grads_in()
    reduce(2)
    route_home(2)
    route_home(3)
    grads_down()
    collect(2)
    reduce(3)
    reduce(0)
    collect(3)
    collect(0)

    for shift in range(1, splits):
        small_square(shift).wait_recv()
    value = square_mine[...]
    for shift in range(1, splits):
        value = value + peer_square[shift - 1]
    square_out[...] = value
    for step in range(1, GROUPS):
        home_copy(step).wait_recv()
    everything = back[...].reshape(-1, width)
    selector = gsel_ref[...].reshape(everything.shape[0], -1)
    token_out[...] = lax.dot_general(
        selector, everything, (((0,), (0,)), ((), ())), preferred_element_type=f32
    ).astype(bf16)

    for step in range(GROUPS):
        if step:
            home_copy(step).wait_send()
            for i in range(3):
                far_copy(step, i).wait_send()

        @pl.loop(1, members)
        def _(hop):
            for i in range(2):
                near_copy(step, hop, i).wait_send()
            join_copy(step, hop).wait_send()

        @pl.loop(0, members)
        def _(hop):
            for shift in range(1, splits):
                swap(step, hop, shift).wait_send()

        @pl.loop(0 if step else 1, members)
        def _(hop):
            for shift in range(1, splits):
                for i in range(2):
                    relay(step, hop, shift, i, col).wait_send()
            scale_copy(step, hop).wait_send()
            route_copy(step, hop).wait()

        for shift in range(1, splits):
            small_route(step, shift).wait_send()
    for shift in range(1, splits):
        small_square(shift).wait_send()


def layer(tokens, cot, gsel, choice, scale, gate, up, down, experts, splits):
    members = experts // GROUPS
    tok_rows, model_width = tokens.shape
    group_cap, span = choice.shape[1:]
    capacity = span // members
    hidden_width = gate.shape[1]
    width = model_width // splits
    window = max(w for _, w in column_plan(model_width, splits))
    f32, bf16 = jnp.float32, jnp.bfloat16
    vmem = pl.BlockSpec(memory_space=pltpu.VMEM)
    hbm = pl.BlockSpec(memory_space=pl.ANY)
    dma = pltpu.SemaphoreType.DMA
    shape = jax.ShapeDtypeStruct
    slots = (GROUPS, members, capacity)
    return pl.pallas_call(
        functools.partial(layer_kernel, experts, splits),
        out_shape=(
            shape((tok_rows, width), bf16),
            shape((experts, 1, span), f32),
            shape((model_width, hidden_width), bf16),
            shape((model_width, hidden_width), bf16),
            shape((2, 1, model_width), f32),
            shape((hidden_width, model_width), bf16),
            shape((1, hidden_width), f32),
        ),
        in_specs=[vmem] * 5 + [hbm] * 3,
        out_specs=(vmem,) * 7,
        scratch_shapes=[
            pltpu.VMEM((2, GROUPS, group_cap, window), bf16),
            pltpu.VMEM((2, GROUPS, group_cap, window), bf16),
            pltpu.VMEM((GROUPS, group_cap, span), bf16),
            pltpu.VMEM((2,) + slots + (model_width,), bf16),
            pltpu.VMEM((2,) + slots + (model_width,), bf16),
            pltpu.VMEM((GROUPS, members, 1, LANES), f32),
            pltpu.VMEM((model_width, 2 * hidden_width), bf16),
            pltpu.VMEM((hidden_width, model_width), bf16),
            pltpu.VMEM((GROUPS * span, 2 * hidden_width), bf16),
            pltpu.VMEM((GROUPS * span, hidden_width), bf16),
            pltpu.VMEM(slots + (model_width,), bf16),
            pltpu.VMEM((splits - 1,) + slots + (width,), bf16),
            pltpu.VMEM(slots + (width,), bf16),
            pltpu.VMEM(slots + (width,), bf16),
            pltpu.VMEM((GROUPS, group_cap, width), bf16),
            pltpu.VMEM((GROUPS, group_cap, width), bf16),
            pltpu.VMEM((GROUPS, 1, span), f32),
            pltpu.VMEM((splits - 1, GROUPS, 1, span), f32),
            pltpu.VMEM((GROUPS, 1, span), f32),
            pltpu.VMEM((2, 1, model_width), f32),
            pltpu.VMEM((splits - 1, 2, 1, model_width), f32),
            pltpu.VMEM((hidden_width, LANES), f32),
            dma((3, GROUPS)), dma((3, GROUPS)),
            dma((2, GROUPS, members)), dma((2, GROUPS, members)),
            dma((2, splits - 1, GROUPS, members)), dma((2, splits - 1, GROUPS, members)),
            dma((GROUPS, members)), dma((GROUPS, members)),
            dma((splits - 1, GROUPS, members)), dma((splits - 1, GROUPS, members)),
            dma((GROUPS, members)), dma((GROUPS, members)),
            dma((GROUPS,)), dma((GROUPS,)),
            dma((splits - 1, GROUPS)), dma((splits - 1, GROUPS)),
            dma((GROUPS, members)), dma((GROUPS, members)),
            dma((splits - 1,)), dma((splits - 1,)),
            dma((3,)),
        ],
        compiler_params=pltpu.CompilerParams(
            collective_id=0, has_side_effects=True, vmem_limit_bytes=60000 * 1024
        ),
    )(tokens, cot, gsel, choice, scale, gate, up, down)


def on_device(tokens, expert_ids, route_weights, cotangent, w_gate, w_up, w_down):
    tok_rows, model_width = tokens.shape
    topk = expert_ids.shape[1]
    experts = lax.axis_size("ep")
    splits = lax.axis_size("tp")
    capacity = 2 * tok_rows * topk // experts
    slot_count = experts * capacity
    f32, bf16 = jnp.float32, jnp.bfloat16

    expert_iota = jnp.arange(experts, dtype=jnp.int32)[None, :]
    slots = jnp.arange(slot_count, dtype=jnp.int32)[None, :]
    slot_expert = slots // capacity
    spread = (expert_iota.reshape(experts, 1) == slot_expert).astype(bf16)
    picks = [expert_ids[:, k : k + 1] == expert_iota for k in range(topk)]
    member = sum(p.astype(f32) for p in picks)
    weight = sum(
        jnp.where(p, route_weights[:, k : k + 1].astype(f32), 0.0) for k, p in enumerate(picks)
    ).astype(bf16)
    order = jnp.arange(tok_rows, dtype=jnp.int32)
    earlier = (order[:, None] > order[None, :]).astype(bf16)
    before = jnp.dot(earlier, member.astype(bf16), preferred_element_type=f32)
    rank = jnp.where(member > 0, before, -1.0).astype(bf16)
    slot_rank = jnp.dot(rank, spread, preferred_element_type=f32)
    chosen = slot_rank == (slots % capacity).astype(f32)
    select = chosen.astype(bf16)
    slot_weight = jnp.sum(
        jnp.where(chosen, jnp.dot(weight, spread, preferred_element_type=f32), 0.0), axis=0
    )
    members = experts // GROUPS
    group_cap = members * capacity // topk
    group_slots = jnp.arange(GROUPS * group_cap, dtype=jnp.int32)[None, :]
    group_iota = jnp.arange(GROUPS, dtype=jnp.int32)[None, :]
    in_group = expert_ids[:, :1] // members == group_iota
    group_before = jnp.dot(earlier, in_group.astype(bf16), preferred_element_type=f32)
    own_rank = jnp.sum(jnp.where(in_group, group_before, 0.0), axis=1, keepdims=True).astype(jnp.int32)
    own_slot = expert_ids[:, :1] // members * group_cap + own_rank
    group_select = (own_slot == group_slots).astype(bf16)
    grouped = lax.dot_general(
        group_select, select, (((0,), (0,)), ((), ())), preferred_element_type=f32
    ).astype(bf16)
    span = members * capacity
    choice = jnp.stack(
        [
            grouped[g * group_cap : (g + 1) * group_cap, g * span : (g + 1) * span]
            for g in range(GROUPS)
        ]
    )
    gsel = group_select.T.reshape(GROUPS, group_cap, tok_rows)

    lane_pad = -capacity % LANES
    scale_out = jnp.pad(slot_weight.reshape(experts, 1, capacity), ((0, 0), (0, 0), (0, lane_pad)))
    token_grad, back_route, grad_gate, grad_up, squares, grad_down, down_square = layer(
        tokens, cotangent, gsel, choice, scale_out, w_gate[0], w_up[0], w_down[0], experts, splits
    )
    seat = lax.rem(lax.axis_index("ep"), members)
    slot_route = lax.dynamic_slice_in_dim(
        back_route.reshape(experts, members, capacity), seat, 1, 1
    ).reshape(1, slot_count)
    route_grad = jnp.concatenate(
        [
            jnp.sum(
                jnp.where(chosen & (slot_expert == expert_ids[:, k : k + 1]), slot_route, 0.0),
                axis=1, keepdims=True,
            )
            for k in range(topk)
        ],
        axis=1,
    ).astype(bf16)
    return (
        token_grad,
        route_grad,
        grad_gate[None],
        grad_up[None],
        grad_down[None],
        squares[0],
        squares[1],
        down_square,
    )


def solution(mesh):
    return jax.shard_map(
        on_device,
        mesh=mesh,
        in_specs=(
            P("ep", None),
            P("ep", None),
            P("ep", None),
            P("ep", None),
            P("ep", None, "tp"),
            P("ep", None, "tp"),
            P("ep", "tp", None),
        ),
        out_specs=(
            P("ep", "tp"),
            P("ep", None),
            P("ep", None, "tp"),
            P("ep", None, "tp"),
            P("ep", "tp", None),
            P("ep", None),
            P("ep", None),
            P("ep", "tp"),
        ),
        check_vma=False,
    )
```

```python
import functools

import jax
import jax.numpy as jnp
from jax import lax
from jax.experimental import pallas as pl
from jax.experimental.layout import Layout, with_layout_constraint
from jax.experimental.pallas import tpu as pltpu
from jax.sharding import PartitionSpec as P

MESH = pl.DeviceIdType.MESH
LANES = 128
TILE = 256
SHARED = (0, 14, 0, 16)
FIRST_COMPUTE = "compute2"
PLAN = (
    "far21 far20 far10 spread00 forward00 spread01 far11 far31",
    "spread21 forward01 forward21 spread20 far30 spread10 forward20",
    "spread11 forward10 compute2 spread31 forward11 compute0",
    "spread30 forward31 compute1 reduce2 forward30 compute3",
    "reduce0 reduce1 down collect2 reduce3 collect1 collect3 wide collect0",
)
GROUPS = 4


def greet(experts, splits, me, col):
    barrier = pltpu.get_barrier_semaphore()

    @pl.loop(1, experts)
    def _(off):
        pl.semaphore_signal(
            barrier, inc=1, device_id={"ep": lax.rem(me + off, experts), "tp": col}, device_id_type=MESH
        )

    for shift in range(1, splits):
        pl.semaphore_signal(
            barrier, inc=1, device_id={"ep": me, "tp": lax.rem(col + shift, splits)}, device_id_type=MESH
        )
    return barrier


def remote(src, dst, send, recv, ep, tp):
    return pltpu.make_async_remote_copy(
        src_ref=src,
        dst_ref=dst,
        send_sem=send,
        recv_sem=recv,
        device_id={"ep": ep, "tp": tp},
        device_id_type=MESH,
    )


def partner(group, step):
    if step == 0:
        return group
    if step == 1:
        return group + 1 - 2 * lax.rem(group, 2)
    if step == 2:
        return lax.rem(group + 2, GROUPS)
    return GROUPS - 1 - group


def column_plan(model_width, splits):
    plan = []
    for part in SHARED:
        shared = model_width * part // 16 // (splits * LANES) * (splits * LANES) if splits == 2 else 0
        cut = (model_width - shared) // splits
        plan.append((cut, cut + shared))
    return plan


def layer_kernel(
    experts, splits,
    ids_ref, weight_ref, tokens_hbm, cot_hbm, gate_hbm, up_hbm, down_hbm,
    token_out, route_out, gate_out, up_out, gate_square_out, up_square_out, down_out, down_square_out,
    tokens_ref, cot_ref, gsel_ref, choice_ref, scale_ref, back_route, packed, landed, landed_choice, stage, rows, scale_in, wide, down, cots, weighted,
    part, peer_part, total, gathered, finished, back, route_mine, peer_route, route_total,
    square_mine, peer_square, down_acc,
    far_send, far_recv, near_send, near_recv, relay_send, relay_recv, scale_send, scale_recv,
    swap_send, swap_recv, join_send, join_recv, home_send, home_recv, small_send, small_recv,
    route_send, route_recv, square_send, square_recv, local,
):
    me = lax.axis_index("ep")
    col = lax.axis_index("tp")
    members = experts // GROUPS
    group = me // members
    seat = lax.rem(me, members)
    model_width = tokens_ref.shape[1]
    capacity = rows.shape[3]
    span = members * capacity
    hidden_width = down.shape[0]
    width = model_width // splits
    f32, bf16 = jnp.float32, jnp.bfloat16
    plan = column_plan(model_width, splits)
    places = [partner(group, step) for step in range(GROUPS)]
    barrier = greet(experts, splits, me, col)
    inputs = (tokens_ref, cot_ref)

    weight_loads = (
        pltpu.make_async_copy(gate_hbm, wide.at[:, pl.ds(0, hidden_width)], local.at[0]),
        pltpu.make_async_copy(up_hbm, wide.at[:, pl.ds(hidden_width, hidden_width)], local.at[1]),
        pltpu.make_async_copy(down_hbm, down, local.at[2]),
    )
    input_loads = (
        pltpu.make_async_copy(tokens_hbm, tokens_ref, local.at[3]),
        pltpu.make_async_copy(cot_hbm, cot_ref, local.at[4]),
    )
    for load in input_loads + weight_loads:
        load.start()

    def window(step):
        cut, wide_cut = plan[step]
        return pl.ds(pl.multiple_of(col * cut, LANES), wide_cut)

    def relay_part(step, which):
        cut, wide_cut = plan[step]
        return pl.ds(pl.multiple_of(which * wide_cut, LANES), cut)

    def around(hop):
        return lax.rem(seat + hop, members)

    def before(hop):
        return lax.rem(seat + members - hop, members)

    def far_copy(step, i):
        if i == 2:
            source, target = choice_ref.at[places[step]], landed_choice.at[step]
        else:
            cols = pl.ds(0, plan[step][1])
            source, target = packed.at[i, step, :, cols], landed.at[i, step, :, cols]
        return remote(
            source, target, far_send.at[i, step], far_recv.at[i, step],
            places[step] * members + seat, col,
        )

    def scale_copy(step, hop):
        there = places[step] * members + around(hop)
        return remote(
            scale_ref.at[places[step]], scale_in.at[step, seat],
            scale_send.at[step, hop], scale_recv.at[step, hop], there, col,
        )

    mate = seat + 1 - 2 * lax.rem(seat, 2)
    chip = seat - lax.rem(seat, 2)

    def mate_copy(i, hop):
        return remote(
            stage.at[i, 0, mate], rows.at[i, 0, seat], near_send.at[i, 0, hop], near_recv.at[i, 0, hop],
            group * members + mate, col,
        )

    mate_out = lax.rem(mate - seat + members, members)
    mate_in = lax.rem(seat - mate + members, members)

    def each_hop(step, own, outgoing, act):
        if step:
            first = 0 if own else 1

            @pl.loop(first, members)
            def _(hop):
                act(hop)
        else:

            @pl.loop(2, members)
            def _(turn):
                other = lax.rem(chip + turn, members)
                gap = other - seat if outgoing else seat - other
                act(lax.rem(gap + members, members))

    def near_copy(step, hop, i):
        if step == 0:
            source = stage.at[i, 0, around(hop), :, window(0)]
        else:
            source = stage.at[i, step, around(hop), :, pl.ds(0, plan[step][1])]
        return remote(
            source, rows.at[i, step, seat, :, window(step)],
            near_send.at[i, step, hop], near_recv.at[i, step, hop], group * members + around(hop), col,
        )

    def relay(step, hop, shift, i, which):
        block = rows.at[i, step, before(hop), :, relay_part(step, which)]
        return remote(
            block, block, relay_send.at[i, shift - 1, step, hop], relay_recv.at[i, shift - 1, step, hop],
            me, lax.rem(col + shift, splits),
        )

    def swap(step, hop, shift):
        peer = lax.rem(col + shift, splits)
        theirs = pl.ds(pl.multiple_of(peer * width, LANES), width)
        return remote(
            part.at[step, around(hop), :, theirs], peer_part.at[shift - 1, step, around(hop)],
            swap_send.at[shift - 1, step, hop], swap_recv.at[shift - 1, step, hop], me, peer,
        )

    def small_route(step, shift):
        return remote(
            route_mine.at[step], peer_route.at[shift - 1, step],
            small_send.at[shift - 1, step], small_recv.at[shift - 1, step],
            me, lax.rem(col + shift, splits),
        )

    def small_square(shift):
        return remote(
            square_mine, peer_square.at[shift - 1], square_send.at[shift - 1], square_recv.at[shift - 1],
            me, lax.rem(col + shift, splits),
        )

    def join_copy(step, hop):
        return remote(
            total.at[step, hop], gathered.at[step, seat],
            join_send.at[step, hop], join_recv.at[step, hop], group * members + around(hop), col,
        )

    def home_copy(step):
        return remote(
            finished.at[step], back.at[group], home_send.at[step], home_recv.at[step],
            places[step] * members + seat, col,
        )

    def route_copy(step, hop):
        there = places[step] * members + around(hop)
        return remote(
            route_total.at[step], back_route.at[me], route_send.at[step, hop], route_recv.at[step, hop],
            there, col,
        )

    def pack(step, i):
        source = inputs[i][:, window(step)] if step else inputs[i][...]
        return jnp.dot(gsel_ref[places[step]], source, preferred_element_type=f32).astype(bf16)

    def spread(step, i, block):
        choice = landed_choice[step] if step else choice_ref[group]
        value = lax.dot_general(choice, block, (((0,), (0,)), ((), ())), preferred_element_type=f32)
        wide_cut = block.shape[1]
        stage[i, step, :, :, pl.ds(0, wide_cut)] = value.astype(bf16).reshape(members, capacity, wide_cut)
        if step == 0:
            mate_copy(i, mate_out).start()
        each_hop(step, False, True, lambda hop: near_copy(step, hop, i).start())

        cols = window(step) if step else pl.ds(0, wide_cut)
        rows[i, step, seat, :, cols] = stage[i, step, seat, :, pl.ds(0, wide_cut)]
        if step:
            for shift in relays(step):
                relay(step, 0, shift, i, col).start()

    def relays(step):
        return range(1, splits) if plan[step][0] else ()

    choices = set()

    def arrive(step, i):
        if step not in choices:
            choices.add(step)
            far_copy(step, 2).wait_recv()
        far_copy(step, i).wait_recv()
        spread(step, i, landed[i, step, :, pl.ds(0, plan[step][1])])

    def forward(step, i):
        def pass_on(hop):
            near_copy(step, hop, i).wait_recv()
            for shift in relays(step):
                relay(step, hop, shift, i, col).start()

        each_hop(step, False, False, pass_on)
        if step == 0:
            mate_copy(i, mate_in).wait_recv()

    def complete(step):
        def landed_all(hop):
            for shift in relays(step):
                for i in range(2):
                    relay(step, hop, shift, i, lax.rem(col + splits - shift, splits)).wait_recv()

        each_hop(step, True, False, landed_all)

        @pl.loop(0 if step else 1, members)
        def _(hop):
            scale_copy(step, hop).wait_recv()

    def compute(step):
        slot_rows = rows[0, step].reshape(span, model_width)
        slot_cot = rows[1, step].reshape(span, model_width)
        pre = jnp.dot(slot_rows, wide[...], preferred_element_type=f32)
        gate_pre, up_pre = pre[:, :hidden_width], pre[:, hidden_width:]
        hidden_back = lax.dot_general(
            slot_cot, down[...], (((1,), (1,)), ((), ())), preferred_element_type=f32
        )
        spread_scale = jnp.broadcast_to(scale_in[step], (members, capacity, span))
        lane = lax.broadcasted_iota(jnp.int32, (members, capacity, span), 2)
        slot = lax.broadcasted_iota(jnp.int32, (members, capacity, span), 1) + seat * capacity
        scale = jnp.sum(jnp.where(lane == slot, spread_scale, 0.0), axis=2, keepdims=True)
        scale = scale.reshape(span, 1)
        gate_sig = jax.nn.sigmoid(gate_pre)
        activated = gate_pre * gate_sig
        hidden = activated * up_pre
        route = hidden * hidden_back
        folded = route[:, :LANES]
        for start in range(LANES, hidden_width, LANES):
            folded = folded + route[:, start : start + LANES]
        route_mine[step] = jnp.sum(folded.T, axis=0, keepdims=True)
        hidden_cot = scale * hidden_back
        up_cot = (hidden_cot * activated).astype(bf16)
        gate_cot = (hidden_cot * up_pre * gate_sig * (1.0 + gate_pre * (1.0 - gate_sig))).astype(bf16)
        slots = pl.ds(step * span, span)
        cots[slots, pl.ds(0, hidden_width)] = gate_cot
        cots[slots, pl.ds(hidden_width, hidden_width)] = up_cot
        weighted[slots, :] = (scale * hidden).astype(bf16)
        both = cots[slots, :]

        @pl.loop(0, model_width // (2 * TILE))
        def _(tile):
            cols = pl.ds(pl.multiple_of(tile * 2 * TILE, LANES), 2 * TILE)
            term = lax.dot_general(
                both, wide[cols, :], (((1,), (1,)), ((), ())), preferred_element_type=f32
            )
            part[step, :, :, cols] = term.astype(bf16).reshape(members, capacity, 2 * TILE)

        for shift in range(1, splits):
            small_route(step, shift).start()

    def send_swaps(step):
        @pl.loop(1, members + 1)
        def _(turn):
            for shift in range(1, splits):
                swap(step, lax.rem(turn, members), shift).start()

    def route_home(step):
        value = route_mine[step]
        for shift in range(1, splits):
            small_route(step, shift).wait_recv()
            value = value + peer_route[shift - 1, step]
        route_total[step] = value
        if step == 0:
            back_route[me] = value

        @pl.loop(0 if step else 1, members)
        def _(hop):
            route_copy(step, hop).start()

    def block_total(step, hop):
        source = around(hop)
        for shift in range(1, splits):
            swap(step, hop, shift).wait_recv()
        mine = pl.ds(pl.multiple_of(col * width, LANES), width)
        value = part[step, source, :, mine].astype(f32)
        for shift in range(1, splits):
            value = value + peer_part[shift - 1, step, source].astype(f32)
        return value.astype(bf16)

    def reduce(step):
        @pl.loop(1, members)
        def _(hop):
            total[step, hop] = block_total(step, hop)
            join_copy(step, hop).start()

        gathered[step, seat] = block_total(step, 0)

    def collect(step):
        @pl.loop(1, members)
        def _(hop):
            join_copy(step, hop).wait_recv()

        pairs = gathered[step].reshape(span, width)
        choice = landed_choice[step] if step else choice_ref[group]
        summed = jnp.dot(choice, pairs, preferred_element_type=f32).astype(bf16)
        if step:
            finished[step] = summed
            home_copy(step).start()
        else:
            back[group] = summed

    def lane_sums(value):
        folded = value[:, :LANES]
        for start in range(LANES, value.shape[1], LANES):
            folded = folded + value[:, start : start + LANES]
        return folded

    def grads_in():
        @pl.loop(0, model_width // TILE)
        def _(tile):
            cols = pl.ds(pl.multiple_of(tile * TILE, LANES), TILE)
            left = rows[0, :, :, :, cols].reshape(GROUPS * span, TILE)
            grad = lax.dot_general(
                left, cots[...], (((0,), (0,)), ((), ())), preferred_element_type=f32
            ).astype(bf16)
            for n, out in enumerate((gate_out, up_out)):
                value = grad[:, n * hidden_width : (n + 1) * hidden_width]
                out[cols, :] = value
                square = lane_sums(jnp.square(value.astype(f32)))
                square_mine[n, :, cols] = jnp.sum(square.T, axis=0, keepdims=True)

        for shift in range(1, splits):
            small_square(shift).start()

    def grads_down():
        down_acc[...] = jnp.zeros_like(down_acc)

        @pl.loop(0, model_width // (2 * TILE))
        def _(tile):
            cols = pl.ds(pl.multiple_of(tile * 2 * TILE, LANES), 2 * TILE)
            right = rows[1, :, :, :, cols].reshape(GROUPS * span, 2 * TILE)
            grad = lax.dot_general(
                weighted[...], right, (((0,), (0,)), ((), ())), preferred_element_type=f32
            ).astype(bf16)
            down_out[:, cols] = grad
            down_acc[...] += lane_sums(jnp.square(grad.astype(f32)))

        down_square_out[...] = jnp.sum(down_acc[...].T, axis=0, keepdims=True)

    topk, tok_rows = ids_ref.shape
    group_cap = gsel_ref.shape[1]

    def count(shape, axis):
        return lax.broadcasted_iota(jnp.int32, shape, axis).astype(f32)

    def one_hot(mask):
        return mask.astype(f32).astype(bf16)

    ids = [ids_ref[pl.ds(k, 1), :].astype(f32) for k in range(topk)]
    expert_count = count((experts, tok_rows), 0)
    picks = [(expert_count == value).astype(f32) for value in ids]
    named = sum(picks).astype(bf16)
    earlier = one_hot(count((tok_rows, tok_rows), 0) < count((tok_rows, tok_rows), 1))
    before_it = jnp.dot(named, earlier, preferred_element_type=f32)
    ranks = [jnp.sum(pick * before_it, axis=0, keepdims=True) for pick in picks]
    group_count = count((4 * GROUPS, tok_rows), 0) * members
    in_group = ((ids[0] >= group_count) & (ids[0] < group_count + members)).astype(f32)
    group_before = jnp.dot(in_group.astype(bf16), earlier, preferred_element_type=f32)
    own_rank = jnp.sum(in_group * group_before, axis=0, keepdims=True)
    for g in range(GROUPS):
        inside = (count((group_cap, tok_rows), 0) == own_rank).astype(f32) * in_group[g : g + 1, :]
        gsel_ref[g] = inside.astype(bf16)
        slot_count = count((span, tok_rows), 0) + g * span
        hits = [one_hot(slot_count == value * capacity + rank) for value, rank in zip(ids, ranks)]
        choice_ref[g] = lax.dot_general(
            inside.astype(bf16), sum(hits), (((1,), (1,)), ((), ())), preferred_element_type=f32
        ).astype(bf16)
        scales = sum(
            lax.dot_general(
                jnp.broadcast_to(weight_ref[pl.ds(k, 1), :].astype(f32), (16, tok_rows)).astype(bf16),
                hits[k], (((1,), (1,)), ((), ())), preferred_element_type=f32,
            )
            for k in range(topk)
        )
        scale_ref[g] = scales[:1]

    def route_back():
        table = back_route[...].reshape(experts, span).astype(bf16)
        lane = count((span, tok_rows), 0) - (seat * capacity).astype(f32)
        for k in range(topk):
            found = lax.dot_general(
                table, picks[k].astype(bf16), (((0,), (0,)), ((), ())), preferred_element_type=f32
            )
            chosen = jnp.where(lane == ranks[k], found, 0.0)
            route_out[pl.ds(k, 1), :] = jnp.sum(chosen, axis=0, keepdims=True).astype(bf16)

    started = set()

    def run(token):
        name, digits = token.rstrip("0123456789"), token.lstrip("abcdefghijklmnopqrstuvwxyz")
        step = int(digits[0]) if digits else 0
        i = int(digits[1:]) if digits[1:] else 0
        if name == "far":
            packed[i, step, :, pl.ds(0, plan[step][1])] = pack(step, i)
            if not started:
                pl.semaphore_wait(barrier, experts - 1 + splits - 1)
            if step not in started:
                started.add(step)
                far_copy(step, 2).start()
            far_copy(step, i).start()
        elif name == "spread":
            if step:
                arrive(step, i)
            else:
                spread(step, i, pack(step, i))
        elif name == "forward":
            forward(step, i)
        elif name == "compute":
            complete(step)
            compute(step)
            send_swaps(step)
        elif name == "reduce":
            route_home(step)
            reduce(step)
        elif name == "collect":
            collect(step)
        elif name == "scale":
            scale_in[0, seat] = scale_ref[group]
            for n in range(GROUPS):

                @pl.loop(0 if n else 1, members)
                def _(hop):
                    scale_copy(n, hop).start()
        elif name == "load":
            for load in weight_loads:
                load.wait()
        elif name == "wide":
            grads_in()
        else:
            grads_down()

    for load in input_loads:
        load.wait()
    for line in PLAN:
        for token in line.split():
            if token == "forward00":
                run("scale")
            if token == FIRST_COMPUTE:
                run("load")
            run(token)

    for step in range(GROUPS):

        @pl.loop(0 if step else 1, members)
        def _(hop):
            route_copy(step, hop).wait_recv()

    route_back()
    for shift in range(1, splits):
        small_square(shift).wait_recv()
    value = square_mine[...]
    for shift in range(1, splits):
        value = value + peer_square[shift - 1]
    gate_square_out[...] = value[0]
    up_square_out[...] = value[1]
    for step in range(1, GROUPS):
        home_copy(step).wait_recv()
    everything = back[...].reshape(-1, width)
    selector = gsel_ref[...].reshape(everything.shape[0], -1)
    token_out[...] = lax.dot_general(
        selector, everything, (((0,), (0,)), ((), ())), preferred_element_type=f32
    ).astype(bf16)

    for step in range(GROUPS):
        if step:
            home_copy(step).wait_send()
            for i in range(3):
                far_copy(step, i).wait_send()

        for i in range(2):
            each_hop(step, False, True, lambda hop: near_copy(step, hop, i).wait_send())
            if step == 0:
                mate_copy(i, mate_out).wait_send()

        @pl.loop(1, members)
        def _(hop):
            join_copy(step, hop).wait_send()

        def relays_sent(hop):
            for shift in relays(step):
                for i in range(2):
                    relay(step, hop, shift, i, col).wait_send()

        each_hop(step, True, False, relays_sent)

        @pl.loop(0, members)
        def _(hop):
            for shift in range(1, splits):
                swap(step, hop, shift).wait_send()

        @pl.loop(0 if step else 1, members)
        def _(hop):
            scale_copy(step, hop).wait_send()
            route_copy(step, hop).wait_send()

        for shift in range(1, splits):
            small_route(step, shift).wait_send()
    for shift in range(1, splits):
        small_square(shift).wait_send()


def layer(ids, weights, tokens, cot, gate, up, down, experts, splits):
    members = experts // GROUPS
    topk, tok_rows = ids.shape
    model_width = tokens.shape[1]
    capacity = 2 * tok_rows * topk // experts
    span = members * capacity
    group_cap = span // topk
    hidden_width = gate.shape[1]
    width = model_width // splits
    window = max(w for _, w in column_plan(model_width, splits))
    f32, bf16 = jnp.float32, jnp.bfloat16
    vmem = pl.BlockSpec(memory_space=pltpu.VMEM)
    hbm = pl.BlockSpec(memory_space=pltpu.HBM)
    dma = pltpu.SemaphoreType.DMA
    shape = jax.ShapeDtypeStruct
    slots = (GROUPS, members, capacity)
    return pl.pallas_call(
        functools.partial(layer_kernel, experts, splits),
        out_shape=(
            shape((tok_rows, width), bf16),
            shape((topk, tok_rows), bf16),
            shape((model_width, hidden_width), bf16),
            shape((model_width, hidden_width), bf16),
            shape((1, model_width), f32),
            shape((1, model_width), f32),
            shape((hidden_width, model_width), bf16),
            shape((1, hidden_width), f32),
        ),
        in_specs=[vmem] * 2 + [hbm] * 5,
        out_specs=(vmem,) * 8,
        scratch_shapes=[
            pltpu.VMEM((tok_rows, model_width), bf16),
            pltpu.VMEM((tok_rows, model_width), bf16),
            pltpu.VMEM((GROUPS, group_cap, tok_rows), bf16),
            pltpu.VMEM((GROUPS, group_cap, span), bf16),
            pltpu.VMEM((GROUPS, 1, span), f32),
            pltpu.VMEM((experts, 1, span), f32),
            pltpu.VMEM((2, GROUPS, group_cap, window), bf16),
            pltpu.VMEM((2, GROUPS, group_cap, window), bf16),
            pltpu.VMEM((GROUPS, group_cap, span), bf16),
            pltpu.VMEM((2,) + slots + (model_width,), bf16),
            pltpu.VMEM((2,) + slots + (model_width,), bf16),
            pltpu.VMEM((GROUPS, members, 1, span), f32),
            pltpu.VMEM((model_width, 2 * hidden_width), bf16),
            pltpu.VMEM((hidden_width, model_width), bf16),
            pltpu.VMEM((GROUPS * span, 2 * hidden_width), bf16),
            pltpu.VMEM((GROUPS * span, hidden_width), bf16),
            pltpu.VMEM(slots + (model_width,), bf16),
            pltpu.VMEM((splits - 1,) + slots + (width,), bf16),
            pltpu.VMEM(slots + (width,), bf16),
            pltpu.VMEM(slots + (width,), bf16),
            pltpu.VMEM((GROUPS, group_cap, width), bf16),
            pltpu.VMEM((GROUPS, group_cap, width), bf16),
            pltpu.VMEM((GROUPS, 1, span), f32),
            pltpu.VMEM((splits - 1, GROUPS, 1, span), f32),
            pltpu.VMEM((GROUPS, 1, span), f32),
            pltpu.VMEM((2, 1, model_width), f32),
            pltpu.VMEM((splits - 1, 2, 1, model_width), f32),
            pltpu.VMEM((hidden_width, LANES), f32),
            dma((3, GROUPS)), dma((3, GROUPS)),
            dma((2, GROUPS, members)), dma((2, GROUPS, members)),
            dma((2, splits - 1, GROUPS, members)), dma((2, splits - 1, GROUPS, members)),
            dma((GROUPS, members)), dma((GROUPS, members)),
            dma((splits - 1, GROUPS, members)), dma((splits - 1, GROUPS, members)),
            dma((GROUPS, members)), dma((GROUPS, members)),
            dma((GROUPS,)), dma((GROUPS,)),
            dma((splits - 1, GROUPS)), dma((splits - 1, GROUPS)),
            dma((GROUPS, members)), dma((GROUPS, members)),
            dma((splits - 1,)), dma((splits - 1,)),
            dma((5,)),
        ],
        compiler_params=pltpu.CompilerParams(
            collective_id=0, has_side_effects=True, vmem_limit_bytes=50000 * 1024
        ),
    )(ids, weights, tokens, cot, gate, up, down)


def export_kernel(*refs):
    count = len(refs) // 2
    copies = [
        pltpu.make_async_copy(refs[n], refs[count + n], refs[-1].at[n]) for n in range(count)
    ]
    for copy in copies:
        copy.start()
    for copy in copies:
        copy.wait()


def export(arrays):
    return pl.pallas_call(
        export_kernel,
        out_shape=tuple(jax.ShapeDtypeStruct(a.shape, a.dtype) for a in arrays),
        in_specs=[pl.BlockSpec(memory_space=pltpu.VMEM)] * len(arrays),
        out_specs=(pl.BlockSpec(memory_space=pltpu.HBM),) * len(arrays),
        scratch_shapes=[pltpu.SemaphoreType.DMA((len(arrays),))],
        compiler_params=pltpu.CompilerParams(vmem_limit_bytes=8000 * 1024),
    )(*arrays)


def on_device(tokens, expert_ids, route_weights, cotangent, w_gate, w_up, w_down):
    experts = lax.axis_size("ep")
    splits = lax.axis_size("tp")
    results = layer(
        expert_ids.T, route_weights.T, tokens, cotangent, w_gate[0], w_up[0], w_down[0], experts, splits
    )
    token_grad, route_grad, grad_gate, grad_up, gate_square, up_square, grad_down, down_square = export(results)
    return (
        token_grad,
        route_grad.T,
        grad_gate[None],
        grad_up[None],
        grad_down[None],
        gate_square,
        up_square,
        down_square,
    )


def solution(mesh):
    return jax.shard_map(
        on_device,
        mesh=mesh,
        in_specs=(
            P("ep", None),
            P("ep", None),
            P("ep", None),
            P("ep", None),
            P("ep", None, "tp"),
            P("ep", None, "tp"),
            P("ep", "tp", None),
        ),
        out_specs=(
            P("ep", "tp"),
            P("ep", None),
            P("ep", None, "tp"),
            P("ep", None, "tp"),
            P("ep", "tp", None),
            P("ep", None),
            P("ep", None),
            P("ep", "tp"),
        ),
        check_vma=False,
    )
```

```python
import functools

import jax
import jax.numpy as jnp
from jax import lax
from jax.experimental import pallas as pl
from jax.experimental.layout import Layout, with_layout_constraint
from jax.experimental.pallas import tpu as pltpu
from jax.sharding import PartitionSpec as P

MESH = pl.DeviceIdType.MESH
LANES = 128
TILE = 256
SHARED = (0, 14, 0, 16)
FIRST_COMPUTE = "compute2"
PLAN = (
    "far21", "far20", "far10", "spread00", "forward00", "spread01", "far11", "far31", "spread21",
    "forward01", "forward21", "spread20", "far30", "spread10", "forward20", "spread11", "forward10",
    "compute2", "spread31", "forward11", "compute0", "spread30", "forward31", "compute1", "reduce2",
    "forward30", "compute3", "reduce0", "reduce1", "down", "collect2", "reduce3", "collect1",
    "collect3", "wide", "collect0",
)
GROUPS = 4


def greet(experts, splits, me, col):
    barrier = pltpu.get_barrier_semaphore()

    @pl.loop(1, experts)
    def _(off):
        pl.semaphore_signal(
            barrier, inc=1, device_id={"ep": lax.rem(me + off, experts), "tp": col}, device_id_type=MESH
        )

    for shift in range(1, splits):
        pl.semaphore_signal(
            barrier, inc=1, device_id={"ep": me, "tp": lax.rem(col + shift, splits)}, device_id_type=MESH
        )
    return barrier


def remote(src, dst, send, recv, ep, tp):
    return pltpu.make_async_remote_copy(
        src_ref=src,
        dst_ref=dst,
        send_sem=send,
        recv_sem=recv,
        device_id={"ep": ep, "tp": tp},
        device_id_type=MESH,
    )


def partner(group, step):
    if step == 0:
        return group
    if step == 1:
        return group + 1 - 2 * lax.rem(group, 2)
    if step == 2:
        return lax.rem(group + 2, GROUPS)
    return GROUPS - 1 - group


def column_plan(model_width, splits):
    plan = []
    for part in SHARED:
        shared = model_width * part // 16 // (splits * LANES) * (splits * LANES) if splits == 2 else 0
        cut = (model_width - shared) // splits
        plan.append((cut, cut + shared))
    return plan


def layer_kernel(
    experts, splits,
    ids_ref, weight_ref, tokens_hbm, cot_hbm, gate_hbm, up_hbm, down_hbm,
    token_out, route_out, gate_out, up_out, gate_square_out, up_square_out, down_out, down_square_out,
    tokens_ref, cot_ref, gsel_ref, choice_ref, scale_ref, back_route, packed, landed, landed_choice, stage, rows, scale_in, wide, down, cots, weighted,
    part, peer_part, total, gathered, finished, back, route_mine, peer_route, route_total,
    square_mine, peer_square, down_acc,
    far_send, far_recv, near_send, near_recv, relay_send, relay_recv, scale_send, scale_recv,
    swap_send, swap_recv, join_send, join_recv, home_send, home_recv, small_send, small_recv,
    route_send, route_recv, square_send, square_recv, local,
):
    me = lax.axis_index("ep")
    col = lax.axis_index("tp")
    members = experts // GROUPS
    group = me // members
    seat = lax.rem(me, members)
    model_width = tokens_ref.shape[1]
    capacity = rows.shape[3]
    span = members * capacity
    hidden_width = down.shape[0]
    width = model_width // splits
    f32, bf16 = jnp.float32, jnp.bfloat16
    plan = column_plan(model_width, splits)
    places = [partner(group, step) for step in range(GROUPS)]
    barrier = greet(experts, splits, me, col)
    inputs = (tokens_ref, cot_ref)

    weight_loads = (
        pltpu.make_async_copy(gate_hbm, wide.at[:, pl.ds(0, hidden_width)], local.at[0]),
        pltpu.make_async_copy(up_hbm, wide.at[:, pl.ds(hidden_width, hidden_width)], local.at[1]),
        pltpu.make_async_copy(down_hbm, down, local.at[2]),
    )
    input_loads = (
        pltpu.make_async_copy(tokens_hbm, tokens_ref, local.at[3]),
        pltpu.make_async_copy(cot_hbm, cot_ref, local.at[4]),
    )
    for load in input_loads + weight_loads:
        load.start()

    def window(step):
        cut, wide_cut = plan[step]
        return pl.ds(pl.multiple_of(col * cut, LANES), wide_cut)

    def relay_part(step, which):
        cut, wide_cut = plan[step]
        return pl.ds(pl.multiple_of(which * wide_cut, LANES), cut)

    def around(hop):
        return lax.rem(seat + hop, members)

    def before(hop):
        return lax.rem(seat + members - hop, members)

    def far_copy(step, i):
        if i == 2:
            source, target = choice_ref.at[places[step]], landed_choice.at[step]
        else:
            cols = pl.ds(0, plan[step][1])
            source, target = packed.at[i, step, :, cols], landed.at[i, step, :, cols]
        return remote(
            source, target, far_send.at[i, step], far_recv.at[i, step],
            places[step] * members + seat, col,
        )

    def scale_copy(step, hop):
        there = places[step] * members + around(hop)
        return remote(
            scale_ref.at[places[step]], scale_in.at[step, seat],
            scale_send.at[step, hop], scale_recv.at[step, hop], there, col,
        )

    mate = seat + 1 - 2 * lax.rem(seat, 2)
    chip = seat - lax.rem(seat, 2)

    def mate_copy(i, hop):
        return remote(
            stage.at[i, 0, mate], rows.at[i, 0, seat], near_send.at[i, 0, hop], near_recv.at[i, 0, hop],
            group * members + mate, col,
        )

    mate_out = lax.rem(mate - seat + members, members)
    mate_in = lax.rem(seat - mate + members, members)

    def each_hop(step, own, outgoing, act):
        if step:
            first = 0 if own else 1

            @pl.loop(first, members)
            def _(hop):
                act(hop)
        else:

            @pl.loop(2, members)
            def _(turn):
                other = lax.rem(chip + turn, members)
                gap = other - seat if outgoing else seat - other
                act(lax.rem(gap + members, members))

    def near_copy(step, hop, i):
        if step == 0:
            source = stage.at[i, 0, around(hop), :, window(0)]
        else:
            source = stage.at[i, step, around(hop), :, pl.ds(0, plan[step][1])]
        return remote(
            source, rows.at[i, step, seat, :, window(step)],
            near_send.at[i, step, hop], near_recv.at[i, step, hop], group * members + around(hop), col,
        )

    def relay(step, hop, shift, i, which):
        block = rows.at[i, step, before(hop), :, relay_part(step, which)]
        return remote(
            block, block, relay_send.at[i, shift - 1, step, hop], relay_recv.at[i, shift - 1, step, hop],
            me, lax.rem(col + shift, splits),
        )

    def swap(step, hop, shift):
        peer = lax.rem(col + shift, splits)
        theirs = pl.ds(pl.multiple_of(peer * width, LANES), width)
        return remote(
            part.at[step, around(hop), :, theirs], peer_part.at[shift - 1, step, around(hop)],
            swap_send.at[shift - 1, step, hop], swap_recv.at[shift - 1, step, hop], me, peer,
        )

    def small_route(step, shift):
        return remote(
            route_mine.at[step], peer_route.at[shift - 1, step],
            small_send.at[shift - 1, step], small_recv.at[shift - 1, step],
            me, lax.rem(col + shift, splits),
        )

    def small_square(shift):
        return remote(
            square_mine, peer_square.at[shift - 1], square_send.at[shift - 1], square_recv.at[shift - 1],
            me, lax.rem(col + shift, splits),
        )

    def join_copy(step, hop):
        return remote(
            total.at[step, hop], gathered.at[step, seat],
            join_send.at[step, hop], join_recv.at[step, hop], group * members + around(hop), col,
        )

    def home_copy(step):
        return remote(
            finished.at[step], back.at[group], home_send.at[step], home_recv.at[step],
            places[step] * members + seat, col,
        )

    def route_copy(step, hop):
        there = places[step] * members + around(hop)
        return remote(
            route_total.at[step], back_route.at[me], route_send.at[step, hop], route_recv.at[step, hop],
            there, col,
        )

    def pack(step, i):
        source = inputs[i][:, window(step)] if step else inputs[i][...]
        return jnp.dot(gsel_ref[places[step]], source, preferred_element_type=f32).astype(bf16)

    def spread(step, i, block):
        choice = landed_choice[step] if step else choice_ref[group]
        value = lax.dot_general(choice, block, (((0,), (0,)), ((), ())), preferred_element_type=f32)
        wide_cut = block.shape[1]
        stage[i, step, :, :, pl.ds(0, wide_cut)] = value.astype(bf16).reshape(members, capacity, wide_cut)
        if step == 0:
            mate_copy(i, mate_out).start()
        each_hop(step, False, True, lambda hop: near_copy(step, hop, i).start())

        cols = window(step) if step else pl.ds(0, wide_cut)
        rows[i, step, seat, :, cols] = stage[i, step, seat, :, pl.ds(0, wide_cut)]
        if step:
            for shift in relays(step):
                relay(step, 0, shift, i, col).start()

    def relays(step):
        return range(1, splits) if plan[step][0] else ()

    choices = set()

    def arrive(step, i):
        if step not in choices:
            choices.add(step)
            far_copy(step, 2).wait_recv()
        far_copy(step, i).wait_recv()
        spread(step, i, landed[i, step, :, pl.ds(0, plan[step][1])])

    def forward(step, i):
        def pass_on(hop):
            near_copy(step, hop, i).wait_recv()
            for shift in relays(step):
                relay(step, hop, shift, i, col).start()

        each_hop(step, False, False, pass_on)
        if step == 0:
            mate_copy(i, mate_in).wait_recv()

    def complete(step):
        def landed_all(hop):
            for shift in relays(step):
                for i in range(2):
                    relay(step, hop, shift, i, lax.rem(col + splits - shift, splits)).wait_recv()

        each_hop(step, True, False, landed_all)

        @pl.loop(0 if step else 1, members)
        def _(hop):
            scale_copy(step, hop).wait_recv()

    def compute(step):
        slot_rows = rows[0, step].reshape(span, model_width)
        slot_cot = rows[1, step].reshape(span, model_width)
        pre = jnp.dot(slot_rows, wide[...], preferred_element_type=f32)
        gate_pre, up_pre = pre[:, :hidden_width], pre[:, hidden_width:]
        hidden_back = lax.dot_general(
            slot_cot, down[...], (((1,), (1,)), ((), ())), preferred_element_type=f32
        )
        spread_scale = jnp.broadcast_to(scale_in[step], (members, capacity, span))
        lane = lax.broadcasted_iota(jnp.int32, (members, capacity, span), 2)
        slot = lax.broadcasted_iota(jnp.int32, (members, capacity, span), 1) + seat * capacity
        scale = jnp.sum(jnp.where(lane == slot, spread_scale, 0.0), axis=2, keepdims=True)
        scale = scale.reshape(span, 1)
        gate_sig = jax.nn.sigmoid(gate_pre)
        activated = gate_pre * gate_sig
        hidden = activated * up_pre
        route = hidden * hidden_back
        folded = route[:, :LANES]
        for start in range(LANES, hidden_width, LANES):
            folded = folded + route[:, start : start + LANES]
        route_mine[step] = jnp.sum(folded.T, axis=0, keepdims=True)
        hidden_cot = scale * hidden_back
        up_cot = (hidden_cot * activated).astype(bf16)
        gate_cot = (hidden_cot * up_pre * gate_sig * (1.0 + gate_pre * (1.0 - gate_sig))).astype(bf16)
        slots = pl.ds(step * span, span)
        cots[slots, pl.ds(0, hidden_width)] = gate_cot
        cots[slots, pl.ds(hidden_width, hidden_width)] = up_cot
        weighted[slots, :] = (scale * hidden).astype(bf16)
        both = cots[slots, :]

        @pl.loop(0, model_width // (2 * TILE))
        def _(tile):
            cols = pl.ds(pl.multiple_of(tile * 2 * TILE, LANES), 2 * TILE)
            term = lax.dot_general(
                both, wide[cols, :], (((1,), (1,)), ((), ())), preferred_element_type=f32
            )
            part[step, :, :, cols] = term.astype(bf16).reshape(members, capacity, 2 * TILE)

        for shift in range(1, splits):
            small_route(step, shift).start()

    def send_swaps(step):
        @pl.loop(1, members + 1)
        def _(turn):
            for shift in range(1, splits):
                swap(step, lax.rem(turn, members), shift).start()

    def route_home(step):
        value = route_mine[step]
        for shift in range(1, splits):
            small_route(step, shift).wait_recv()
            value = value + peer_route[shift - 1, step]
        route_total[step] = value
        if step == 0:
            back_route[me] = value

        @pl.loop(0 if step else 1, members)
        def _(hop):
            route_copy(step, hop).start()

    def block_total(step, hop):
        source = around(hop)
        for shift in range(1, splits):
            swap(step, hop, shift).wait_recv()
        mine = pl.ds(pl.multiple_of(col * width, LANES), width)
        value = part[step, source, :, mine].astype(f32)
        for shift in range(1, splits):
            value = value + peer_part[shift - 1, step, source].astype(f32)
        return value.astype(bf16)

    def reduce(step):
        @pl.loop(1, members)
        def _(hop):
            total[step, hop] = block_total(step, hop)
            join_copy(step, hop).start()

        gathered[step, seat] = block_total(step, 0)

    def collect(step):
        @pl.loop(1, members)
        def _(hop):
            join_copy(step, hop).wait_recv()

        pairs = gathered[step].reshape(span, width)
        choice = landed_choice[step] if step else choice_ref[group]
        summed = jnp.dot(choice, pairs, preferred_element_type=f32).astype(bf16)
        if step:
            finished[step] = summed
            home_copy(step).start()
        else:
            back[group] = summed

    def lane_sums(value):
        folded = value[:, :LANES]
        for start in range(LANES, value.shape[1], LANES):
            folded = folded + value[:, start : start + LANES]
        return folded

    def grads_in():
        @pl.loop(0, model_width // TILE)
        def _(tile):
            cols = pl.ds(pl.multiple_of(tile * TILE, LANES), TILE)
            left = rows[0, :, :, :, cols].reshape(GROUPS * span, TILE)
            grad = lax.dot_general(
                left, cots[...], (((0,), (0,)), ((), ())), preferred_element_type=f32
            ).astype(bf16)
            for n, out in enumerate((gate_out, up_out)):
                value = grad[:, n * hidden_width : (n + 1) * hidden_width]
                out[cols, :] = value
                square = lane_sums(jnp.square(value.astype(f32)))
                square_mine[n, :, cols] = jnp.sum(square.T, axis=0, keepdims=True)

        for shift in range(1, splits):
            small_square(shift).start()

    def grads_down():
        down_acc[...] = jnp.zeros_like(down_acc)

        @pl.loop(0, model_width // (2 * TILE))
        def _(tile):
            cols = pl.ds(pl.multiple_of(tile * 2 * TILE, LANES), 2 * TILE)
            right = rows[1, :, :, :, cols].reshape(GROUPS * span, 2 * TILE)
            grad = lax.dot_general(
                weighted[...], right, (((0,), (0,)), ((), ())), preferred_element_type=f32
            ).astype(bf16)
            down_out[:, cols] = grad
            down_acc[...] += lane_sums(jnp.square(grad.astype(f32)))

        down_square_out[...] = jnp.sum(down_acc[...].T, axis=0, keepdims=True)

    topk, tok_rows = ids_ref.shape
    group_cap = gsel_ref.shape[1]

    def count(shape, axis):
        return lax.broadcasted_iota(jnp.int32, shape, axis).astype(f32)

    def one_hot(mask):
        return mask.astype(f32).astype(bf16)

    ids = [ids_ref[pl.ds(k, 1), :].astype(f32) for k in range(topk)]
    expert_count = count((experts, tok_rows), 0)
    picks = [(expert_count == value).astype(f32) for value in ids]
    named = sum(picks).astype(bf16)
    earlier = one_hot(count((tok_rows, tok_rows), 0) < count((tok_rows, tok_rows), 1))
    before_it = jnp.dot(named, earlier, preferred_element_type=f32)
    ranks = [jnp.sum(pick * before_it, axis=0, keepdims=True) for pick in picks]
    group_count = count((4 * GROUPS, tok_rows), 0) * members
    in_group = ((ids[0] >= group_count) & (ids[0] < group_count + members)).astype(f32)
    group_before = jnp.dot(in_group.astype(bf16), earlier, preferred_element_type=f32)
    own_rank = jnp.sum(in_group * group_before, axis=0, keepdims=True)
    for g in range(GROUPS):
        inside = (count((group_cap, tok_rows), 0) == own_rank).astype(f32) * in_group[g : g + 1, :]
        gsel_ref[g] = inside.astype(bf16)
        slot_count = count((span, tok_rows), 0) + g * span
        hits = [one_hot(slot_count == value * capacity + rank) for value, rank in zip(ids, ranks)]
        choice_ref[g] = lax.dot_general(
            inside.astype(bf16), sum(hits), (((1,), (1,)), ((), ())), preferred_element_type=f32
        ).astype(bf16)
        scales = sum(
            lax.dot_general(
                jnp.broadcast_to(weight_ref[pl.ds(k, 1), :].astype(f32), (16, tok_rows)).astype(bf16),
                hits[k], (((1,), (1,)), ((), ())), preferred_element_type=f32,
            )
            for k in range(topk)
        )
        scale_ref[g] = scales[:1]

    def route_back():
        table = back_route[...].reshape(experts, span).astype(bf16)
        lane = count((span, tok_rows), 0) - (seat * capacity).astype(f32)
        for k in range(topk):
            found = lax.dot_general(
                table, picks[k].astype(bf16), (((0,), (0,)), ((), ())), preferred_element_type=f32
            )
            chosen = jnp.where(lane == ranks[k], found, 0.0)
            route_out[pl.ds(k, 1), :] = jnp.sum(chosen, axis=0, keepdims=True).astype(bf16)

    started = set()

    def run(token):
        name, digits = token.rstrip("0123456789"), token.lstrip("abcdefghijklmnopqrstuvwxyz")
        step = int(digits[0]) if digits else 0
        i = int(digits[1:]) if digits[1:] else 0
        if name == "far":
            packed[i, step, :, pl.ds(0, plan[step][1])] = pack(step, i)
            if not started:
                pl.semaphore_wait(barrier, experts - 1 + splits - 1)
            if step not in started:
                started.add(step)
                far_copy(step, 2).start()
            far_copy(step, i).start()
        elif name == "spread":
            if step:
                arrive(step, i)
            else:
                spread(step, i, pack(step, i))
        elif name == "forward":
            forward(step, i)
        elif name == "compute":
            complete(step)
            compute(step)
            send_swaps(step)
        elif name == "reduce":
            route_home(step)
            reduce(step)
        elif name == "collect":
            collect(step)
        elif name == "scale":
            scale_in[0, seat] = scale_ref[group]
            for n in range(GROUPS):

                @pl.loop(0 if n else 1, members)
                def _(hop):
                    scale_copy(n, hop).start()
        elif name == "load":
            for load in weight_loads:
                load.wait()
        elif name == "wide":
            grads_in()
        else:
            grads_down()

    for load in input_loads:
        load.wait()
    for token in PLAN:
        if token == "forward00":
            run("scale")
        if token == FIRST_COMPUTE:
            run("load")
        run(token)

    for step in range(GROUPS):

        @pl.loop(0 if step else 1, members)
        def _(hop):
            route_copy(step, hop).wait_recv()

    route_back()
    for shift in range(1, splits):
        small_square(shift).wait_recv()
    value = square_mine[...]
    for shift in range(1, splits):
        value = value + peer_square[shift - 1]
    gate_square_out[...] = value[0]
    up_square_out[...] = value[1]
    for step in range(1, GROUPS):
        home_copy(step).wait_recv()
    everything = back[...].reshape(-1, width)
    selector = gsel_ref[...].reshape(everything.shape[0], -1)
    token_out[...] = lax.dot_general(
        selector, everything, (((0,), (0,)), ((), ())), preferred_element_type=f32
    ).astype(bf16)

    for step in range(GROUPS):
        if step:
            home_copy(step).wait_send()
            for i in range(3):
                far_copy(step, i).wait_send()

        for i in range(2):
            each_hop(step, False, True, lambda hop: near_copy(step, hop, i).wait_send())
            if step == 0:
                mate_copy(i, mate_out).wait_send()

        @pl.loop(1, members)
        def _(hop):
            join_copy(step, hop).wait_send()

        def relays_sent(hop):
            for shift in relays(step):
                for i in range(2):
                    relay(step, hop, shift, i, col).wait_send()

        each_hop(step, True, False, relays_sent)

        @pl.loop(0, members)
        def _(hop):
            for shift in range(1, splits):
                swap(step, hop, shift).wait_send()

        @pl.loop(0 if step else 1, members)
        def _(hop):
            scale_copy(step, hop).wait_send()
            route_copy(step, hop).wait_send()

        for shift in range(1, splits):
            small_route(step, shift).wait_send()
    for shift in range(1, splits):
        small_square(shift).wait_send()


def layer(ids, weights, tokens, cot, gate, up, down, experts, splits):
    members = experts // GROUPS
    topk, tok_rows = ids.shape
    model_width = tokens.shape[1]
    capacity = 2 * tok_rows * topk // experts
    span = members * capacity
    group_cap = span // topk
    hidden_width = gate.shape[1]
    width = model_width // splits
    window = max(w for _, w in column_plan(model_width, splits))
    f32, bf16 = jnp.float32, jnp.bfloat16
    vmem = pl.BlockSpec(memory_space=pltpu.VMEM)
    hbm = pl.BlockSpec(memory_space=pltpu.HBM)
    tokens, cot, gate, up, down = (
        pltpu.with_memory_space_constraint(v, pltpu.HBM) for v in (tokens, cot, gate, up, down)
    )
    dma = pltpu.SemaphoreType.DMA
    shape = jax.ShapeDtypeStruct
    slots = (GROUPS, members, capacity)
    return pl.pallas_call(
        functools.partial(layer_kernel, experts, splits),
        out_shape=(
            shape((tok_rows, width), bf16),
            shape((topk, tok_rows), bf16),
            shape((model_width, hidden_width), bf16),
            shape((model_width, hidden_width), bf16),
            shape((1, model_width), f32),
            shape((1, model_width), f32),
            shape((hidden_width, model_width), bf16),
            shape((1, hidden_width), f32),
        ),
        in_specs=[vmem] * 2 + [hbm] * 5,
        out_specs=(vmem,) * 8,
        scratch_shapes=[
            pltpu.VMEM((tok_rows, model_width), bf16),
            pltpu.VMEM((tok_rows, model_width), bf16),
            pltpu.VMEM((GROUPS, group_cap, tok_rows), bf16),
            pltpu.VMEM((GROUPS, group_cap, span), bf16),
            pltpu.VMEM((GROUPS, 1, span), f32),
            pltpu.VMEM((experts, 1, span), f32),
            pltpu.VMEM((2, GROUPS, group_cap, window), bf16),
            pltpu.VMEM((2, GROUPS, group_cap, window), bf16),
            pltpu.VMEM((GROUPS, group_cap, span), bf16),
            pltpu.VMEM((2,) + slots + (model_width,), bf16),
            pltpu.VMEM((2,) + slots + (model_width,), bf16),
            pltpu.VMEM((GROUPS, members, 1, span), f32),
            pltpu.VMEM((model_width, 2 * hidden_width), bf16),
            pltpu.VMEM((hidden_width, model_width), bf16),
            pltpu.VMEM((GROUPS * span, 2 * hidden_width), bf16),
            pltpu.VMEM((GROUPS * span, hidden_width), bf16),
            pltpu.VMEM(slots + (model_width,), bf16),
            pltpu.VMEM((splits - 1,) + slots + (width,), bf16),
            pltpu.VMEM(slots + (width,), bf16),
            pltpu.VMEM(slots + (width,), bf16),
            pltpu.VMEM((GROUPS, group_cap, width), bf16),
            pltpu.VMEM((GROUPS, group_cap, width), bf16),
            pltpu.VMEM((GROUPS, 1, span), f32),
            pltpu.VMEM((splits - 1, GROUPS, 1, span), f32),
            pltpu.VMEM((GROUPS, 1, span), f32),
            pltpu.VMEM((2, 1, model_width), f32),
            pltpu.VMEM((splits - 1, 2, 1, model_width), f32),
            pltpu.VMEM((hidden_width, LANES), f32),
            dma((3, GROUPS)), dma((3, GROUPS)),
            dma((2, GROUPS, members)), dma((2, GROUPS, members)),
            dma((2, splits - 1, GROUPS, members)), dma((2, splits - 1, GROUPS, members)),
            dma((GROUPS, members)), dma((GROUPS, members)),
            dma((splits - 1, GROUPS, members)), dma((splits - 1, GROUPS, members)),
            dma((GROUPS, members)), dma((GROUPS, members)),
            dma((GROUPS,)), dma((GROUPS,)),
            dma((splits - 1, GROUPS)), dma((splits - 1, GROUPS)),
            dma((GROUPS, members)), dma((GROUPS, members)),
            dma((splits - 1,)), dma((splits - 1,)),
            dma((5,)),
        ],
        compiler_params=pltpu.CompilerParams(
            collective_id=0, has_side_effects=True, vmem_limit_bytes=40000 * 1024
        ),
    )(ids, weights, tokens, cot, gate, up, down)


def export_kernel(*refs):
    count = len(refs) // 2
    copies = [
        pltpu.make_async_copy(refs[n], refs[count + n], refs[-1].at[n]) for n in range(count)
    ]
    for copy in copies:
        copy.start()
    for copy in copies:
        copy.wait()


def export(arrays):
    return pl.pallas_call(
        export_kernel,
        out_shape=tuple(jax.ShapeDtypeStruct(a.shape, a.dtype) for a in arrays),
        in_specs=[pl.BlockSpec(memory_space=pltpu.VMEM)] * len(arrays),
        out_specs=(pl.BlockSpec(memory_space=pltpu.HBM),) * len(arrays),
        scratch_shapes=[pltpu.SemaphoreType.DMA((len(arrays),))],
        compiler_params=pltpu.CompilerParams(vmem_limit_bytes=8000 * 1024),
    )(*arrays)


def on_device(tokens, expert_ids, route_weights, cotangent, w_gate, w_up, w_down):
    experts = lax.axis_size("ep")
    splits = lax.axis_size("tp")
    results = layer(
        expert_ids.T, route_weights.T, tokens, cotangent, w_gate[0], w_up[0], w_down[0], experts, splits
    )
    token_grad, route_grad, grad_gate, grad_up, gate_square, up_square, grad_down, down_square = export(results)
    return (
        token_grad,
        route_grad.T,
        grad_gate[None],
        grad_up[None],
        grad_down[None],
        gate_square,
        up_square,
        down_square,
    )


def solution(mesh):
    return jax.shard_map(
        on_device,
        mesh=mesh,
        in_specs=(
            P("ep", None),
            P("ep", None),
            P("ep", None),
            P("ep", None),
            P("ep", None, "tp"),
            P("ep", None, "tp"),
            P("ep", "tp", None),
        ),
        out_specs=(
            P("ep", "tp"),
            P("ep", None),
            P("ep", None, "tp"),
            P("ep", None, "tp"),
            P("ep", "tp", None),
            P("ep", None),
            P("ep", None),
            P("ep", "tp"),
        ),
        check_vma=False,
    )
```

```python
import functools

import jax
import jax.numpy as jnp
from jax import lax
from jax.experimental import pallas as pl
from jax.experimental.layout import Layout, with_layout_constraint
from jax.experimental.pallas import tpu as pltpu
from jax.sharding import PartitionSpec as P

MESH = pl.DeviceIdType.MESH
LANES = 128
TILE = 256
GROUPS = 4
HALVES = 2
WHOLE = ((0, 1, 0, 0), (1, 1, 1, 1), (0, 0, 0, 0), (1, 1, 0, 1))
PLAN = (
    "far11", "far23", "spread03", "far22", "far21", "spread01", "spread00", "spread02", "fwd03",
    "far12", "spread23", "far20", "spread22", "far10", "fwd01", "far13", "far32", "fwd02", "spread11",
    "fwd22", "far30", "fwd23", "far33", "spread21", "spread20", "fwd00", "spread12", "spread10",
    "fwd20", "fwd21", "fwd11", "spread13", "comp00", "spread32", "comp20", "fwd13", "far31",
    "fwd32", "spread30", "fwd10", "spread33", "fwd12", "comp10", "spread31", "red01", "fwd33",
    "fwd30", "red20", "red21", "fwd31", "comp30", "red10", "grad10", "red00", "col20", "red11",
    "col10", "col21", "red30", "grad30", "red31", "col00", "col30", "col31", "col11", "col01",
    "grad20", "grad00",
)


def greet(experts, splits, me, col):
    barrier = pltpu.get_barrier_semaphore()

    @pl.loop(1, experts)
    def _(off):
        pl.semaphore_signal(
            barrier, inc=1, device_id={"ep": lax.rem(me + off, experts), "tp": col}, device_id_type=MESH
        )

    for shift in range(1, splits):
        pl.semaphore_signal(
            barrier, inc=1, device_id={"ep": me, "tp": lax.rem(col + shift, splits)}, device_id_type=MESH
        )
    return barrier


def remote(src, dst, send, recv, ep, tp):
    return pltpu.make_async_remote_copy(
        src_ref=src,
        dst_ref=dst,
        send_sem=send,
        recv_sem=recv,
        device_id={"ep": ep, "tp": tp},
        device_id_type=MESH,
    )


def partner(group, step):
    if step == 0:
        return group
    if step == 1:
        return group + 1 - 2 * lax.rem(group, 2)
    if step == 2:
        return lax.rem(group + 2, GROUPS)
    return GROUPS - 1 - group


def layer_kernel(
    experts, splits,
    ids_ref, weight_ref, tokens_hbm, cot_hbm, gate_hbm, up_hbm, down_hbm,
    token_out, route_out, gate_out, up_out, gate_square_out, up_square_out, down_out, down_square_out,
    tokens_ref, cot_ref, gsel_ref, choice_ref, scale_ref, back_route, packed, landed, landed_choice, stage, rows, scale_in, wide, down, cots, weighted,
    part, peer_part, total, gathered, finished, back, route_mine, peer_route, route_total,
    square_mine, peer_square, down_acc,
    far_send, far_recv, near_send, near_recv, relay_send, relay_recv, scale_send, scale_recv,
    swap_send, swap_recv, join_send, join_recv, home_send, home_recv, small_send, small_recv,
    route_send, route_recv, square_send, square_recv, local,
):
    me = lax.axis_index("ep")
    col = lax.axis_index("tp")
    members = experts // GROUPS
    group = me // members
    seat = lax.rem(me, members)
    model_width = tokens_ref.shape[1]
    capacity = rows.shape[3]
    span = members * capacity
    hidden_width = down.shape[0]
    width = model_width // splits
    f32, bf16 = jnp.float32, jnp.bfloat16
    halves = peer_part.shape[2]
    half_width = width // halves
    chunk = model_width // halves
    chunks = range(2 * halves)
    places = [partner(group, step) for step in range(GROUPS)]
    barrier = greet(experts, splits, me, col)
    inputs = (tokens_ref, cot_ref)

    weight_loads = (
        pltpu.make_async_copy(gate_hbm, wide.at[:, pl.ds(0, hidden_width)], local.at[0]),
        pltpu.make_async_copy(up_hbm, wide.at[:, pl.ds(hidden_width, hidden_width)], local.at[1]),
        pltpu.make_async_copy(down_hbm, down, local.at[2]),
    )
    input_loads = (
        pltpu.make_async_copy(tokens_hbm, tokens_ref, local.at[3]),
        pltpu.make_async_copy(cot_hbm, cot_ref, local.at[4]),
    )
    for load in input_loads + weight_loads:
        load.start()

    def whole(step, i):
        return WHOLE[step][i * HALVES // halves]

    def chunk_width(step, i):
        return chunk if whole(step, i) else chunk // splits

    def window(step, i):
        base = i % halves * chunk
        if whole(step, i):
            return pl.ds(base, chunk)
        return relay_part(step, i, col)

    def relay_part(step, i, which):
        cut = chunk // splits
        return pl.ds(pl.multiple_of(i % halves * chunk + which * cut, LANES), cut)

    def around(hop):
        return lax.rem(seat + hop, members)

    def before(hop):
        return lax.rem(seat + members - hop, members)

    def far_copy(step, i):
        if i == 2 * halves:
            source, target = choice_ref.at[places[step]], landed_choice.at[step]
        else:
            cols = pl.ds(0, chunk_width(step, i))
            source, target = packed.at[i, step, :, cols], landed.at[i, step, :, cols]
        return remote(
            source, target, far_send.at[i, step], far_recv.at[i, step],
            places[step] * members + seat, col,
        )

    def scale_copy(step, hop):
        there = places[step] * members + around(hop)
        return remote(
            scale_ref.at[places[step]], scale_in.at[step, seat],
            scale_send.at[step, hop], scale_recv.at[step, hop], there, col,
        )

    mate = seat + 1 - 2 * lax.rem(seat, 2)
    chip = seat - lax.rem(seat, 2)

    def mate_copy(i, hop):
        return remote(
            stage.at[i, 0, mate], rows.at[i // halves, 0, seat, :, pl.ds(i % halves * chunk, chunk)], near_send.at[i, 0, hop], near_recv.at[i, 0, hop],
            group * members + mate, col,
        )

    mate_out = lax.rem(mate - seat + members, members)
    mate_in = lax.rem(seat - mate + members, members)

    def each_hop(step, own, outgoing, act):
        if step:
            first = 0 if own else 1

            @pl.loop(first, members)
            def _(hop):
                act(hop)
        else:

            @pl.loop(2, members)
            def _(turn):
                other = lax.rem(chip + turn, members)
                gap = other - seat if outgoing else seat - other
                act(lax.rem(gap + members, members))

    def near_copy(step, hop, i):
        size = chunk_width(step, i)
        start = 0 if step or whole(step, i) else pl.multiple_of(col * size, LANES)
        return remote(
            stage.at[i, step, around(hop), :, pl.ds(start, size)],
            rows.at[i // halves, step, seat, :, window(step, i)],
            near_send.at[i, step, hop], near_recv.at[i, step, hop], group * members + around(hop), col,
        )

    def relay(step, hop, shift, i, which):
        block = rows.at[i // halves, step, before(hop), :, relay_part(step, i, which)]
        return remote(
            block, block, relay_send.at[i, shift - 1, step, hop], relay_recv.at[i, shift - 1, step, hop],
            me, lax.rem(col + shift, splits),
        )

    def swap(step, b, hop, shift):
        peer = lax.rem(col + shift, splits)
        theirs = pl.ds(pl.multiple_of(peer * width + b * half_width, LANES), half_width)
        return remote(
            part.at[step, around(hop), :, theirs], peer_part.at[shift - 1, step, b, around(hop)],
            swap_send.at[shift - 1, step, b, hop], swap_recv.at[shift - 1, step, b, hop], me, peer,
        )

    def small_route(step, shift):
        return remote(
            route_mine.at[step], peer_route.at[shift - 1, step],
            small_send.at[shift - 1, step], small_recv.at[shift - 1, step],
            me, lax.rem(col + shift, splits),
        )

    def small_square(shift):
        return remote(
            square_mine, peer_square.at[shift - 1], square_send.at[shift - 1], square_recv.at[shift - 1],
            me, lax.rem(col + shift, splits),
        )

    def join_copy(step, b, hop):
        return remote(
            total.at[step, b, hop], gathered.at[step, b, seat],
            join_send.at[step, b, hop], join_recv.at[step, b, hop], group * members + around(hop), col,
        )

    def home_copy(step, b):
        return remote(
            finished.at[step, b], back.at[b, group], home_send.at[step, b], home_recv.at[step, b],
            places[step] * members + seat, col,
        )

    def route_copy(step, hop):
        there = places[step] * members + around(hop)
        return remote(
            route_total.at[step], back_route.at[me], route_send.at[step, hop], route_recv.at[step, hop],
            there, col,
        )

    def pack(step, i):
        cols = window(step, i) if step else pl.ds(i % halves * chunk, chunk)
        source = inputs[i // halves][:, cols]
        return jnp.dot(gsel_ref[places[step]], source, preferred_element_type=f32).astype(bf16)

    def spread(step, i, block):
        choice = landed_choice[step] if step else choice_ref[group]
        value = lax.dot_general(choice, block, (((0,), (0,)), ((), ())), preferred_element_type=f32)
        wide_cut = block.shape[1]
        stage[i, step, :, :, pl.ds(0, wide_cut)] = value.astype(bf16).reshape(members, capacity, wide_cut)
        if step == 0:
            mate_copy(i, mate_out).start()
        each_hop(step, False, True, lambda hop: near_copy(step, hop, i).start())

        cols = window(step, i) if step else pl.ds(i % halves * chunk, chunk)
        rows[i // halves, step, seat, :, cols] = stage[i, step, seat, :, pl.ds(0, wide_cut)]
        if step:
            for shift in relays(step, i):
                relay(step, 0, shift, i, col).start()

    def relays(step, i):
        return () if whole(step, i) else range(1, splits)

    choices = set()

    def arrive(step, i):
        if step not in choices:
            choices.add(step)
            far_copy(step, 2 * halves).wait_recv()
        far_copy(step, i).wait_recv()
        spread(step, i, landed[i, step, :, pl.ds(0, chunk_width(step, i))])

    def forward(step, i):
        def pass_on(hop):
            near_copy(step, hop, i).wait_recv()
            for shift in relays(step, i):
                relay(step, hop, shift, i, col).start()

        each_hop(step, False, False, pass_on)
        if step == 0:
            mate_copy(i, mate_in).wait_recv()

    def complete(step):
        def landed_all(hop):
            for i in chunks:
                for shift in relays(step, i):
                    relay(step, hop, shift, i, lax.rem(col + splits - shift, splits)).wait_recv()

        each_hop(step, True, False, landed_all)

        @pl.loop(0 if step else 1, members)
        def _(hop):
            scale_copy(step, hop).wait_recv()

    def compute(step):
        slot_rows = rows[0, step].reshape(span, model_width)
        slot_cot = rows[1, step].reshape(span, model_width)
        pre = jnp.dot(slot_rows, wide[...], preferred_element_type=f32)
        gate_pre, up_pre = pre[:, :hidden_width], pre[:, hidden_width:]
        hidden_back = lax.dot_general(
            slot_cot, down[...], (((1,), (1,)), ((), ())), preferred_element_type=f32
        )
        spread_scale = jnp.broadcast_to(scale_in[step], (members, capacity, span))
        lane = lax.broadcasted_iota(jnp.int32, (members, capacity, span), 2)
        slot = lax.broadcasted_iota(jnp.int32, (members, capacity, span), 1) + seat * capacity
        scale = jnp.sum(jnp.where(lane == slot, spread_scale, 0.0), axis=2, keepdims=True)
        scale = scale.reshape(span, 1)
        gate_sig = jax.nn.sigmoid(gate_pre)
        activated = gate_pre * gate_sig
        hidden = activated * up_pre
        route = hidden * hidden_back
        folded = route[:, :LANES]
        for start in range(LANES, hidden_width, LANES):
            folded = folded + route[:, start : start + LANES]
        route_mine[step] = jnp.sum(folded.T, axis=0, keepdims=True)
        hidden_cot = scale * hidden_back
        up_cot = (hidden_cot * activated).astype(bf16)
        gate_cot = (hidden_cot * up_pre * gate_sig * (1.0 + gate_pre * (1.0 - gate_sig))).astype(bf16)
        slots = pl.ds(step * span, span)
        cots[slots, pl.ds(0, hidden_width)] = gate_cot
        cots[slots, pl.ds(hidden_width, hidden_width)] = up_cot
        weighted[slots, :] = (scale * hidden).astype(bf16)
        both = cots[slots, :]

        @pl.loop(0, model_width // (2 * TILE))
        def _(tile):
            cols = pl.ds(pl.multiple_of(tile * 2 * TILE, LANES), 2 * TILE)
            term = lax.dot_general(
                both, wide[cols, :], (((1,), (1,)), ((), ())), preferred_element_type=f32
            )
            part[step, :, :, cols] = term.astype(bf16).reshape(members, capacity, 2 * TILE)

        for shift in range(1, splits):
            small_route(step, shift).start()

    def send_swaps(step):
        for b in range(halves):

            @pl.loop(1, members + 1)
            def _(turn):
                for shift in range(1, splits):
                    swap(step, b, lax.rem(turn, members), shift).start()

    def route_home(step):
        value = route_mine[step]
        for shift in range(1, splits):
            small_route(step, shift).wait_recv()
            value = value + peer_route[shift - 1, step]
        route_total[step] = value
        if step == 0:
            back_route[me] = value

        @pl.loop(0 if step else 1, members)
        def _(hop):
            route_copy(step, hop).start()

    def block_total(step, b, hop):
        source = around(hop)
        for shift in range(1, splits):
            swap(step, b, hop, shift).wait_recv()
        mine = pl.ds(pl.multiple_of(col * width + b * half_width, LANES), half_width)
        value = part[step, source, :, mine].astype(f32)
        for shift in range(1, splits):
            value = value + peer_part[shift - 1, step, b, source].astype(f32)
        return value.astype(bf16)

    def reduce(step, b):
        @pl.loop(1, members)
        def _(hop):
            total[step, b, hop] = block_total(step, b, hop)
            join_copy(step, b, hop).start()

        gathered[step, b, seat] = block_total(step, b, 0)

    def collect(step, b):
        @pl.loop(1, members)
        def _(hop):
            join_copy(step, b, hop).wait_recv()

        pairs = gathered[step, b].reshape(span, half_width)
        choice = landed_choice[step] if step else choice_ref[group]
        summed = jnp.dot(choice, pairs, preferred_element_type=f32).astype(bf16)
        if step:
            finished[step, b] = summed
            home_copy(step, b).start()
        else:
            back[b, group] = summed

    def lane_sums(value):
        folded = value[:, :LANES]
        for start in range(LANES, value.shape[1], LANES):
            folded = folded + value[:, start : start + LANES]
        return folded

    def grads_in(first):
        tiles = model_width // TILE // 2

        @pl.loop(first * tiles, (first + 1) * tiles)
        def _(tile):
            cols = pl.ds(pl.multiple_of(tile * TILE, LANES), TILE)
            left = rows[0, :, :, :, cols].reshape(GROUPS * span, TILE)
            grad = lax.dot_general(
                left, cots[...], (((0,), (0,)), ((), ())), preferred_element_type=f32
            ).astype(bf16)
            for n, out in enumerate((gate_out, up_out)):
                value = grad[:, n * hidden_width : (n + 1) * hidden_width]
                out[cols, :] = value
                square = lane_sums(jnp.square(value.astype(f32)))
                square_mine[n, :, cols] = jnp.sum(square.T, axis=0, keepdims=True)

    def grads_down(first):
        tiles = model_width // TILE // 4

        @pl.loop(first * tiles, (first + 1) * tiles)
        def _(tile):
            cols = pl.ds(pl.multiple_of(tile * 2 * TILE, LANES), 2 * TILE)
            right = rows[1, :, :, :, cols].reshape(GROUPS * span, 2 * TILE)
            grad = lax.dot_general(
                weighted[...], right, (((0,), (0,)), ((), ())), preferred_element_type=f32
            ).astype(bf16)
            down_out[:, cols] = grad
            down_acc[...] += lane_sums(jnp.square(grad.astype(f32)))

    topk, tok_rows = ids_ref.shape
    group_cap = gsel_ref.shape[1]

    def count(shape, axis):
        return lax.broadcasted_iota(jnp.int32, shape, axis).astype(f32)

    def one_hot(mask):
        return mask.astype(f32).astype(bf16)

    ids = [ids_ref[pl.ds(k, 1), :].astype(f32) for k in range(topk)]
    expert_count = count((experts, tok_rows), 0)
    picks = [(expert_count == value).astype(f32) for value in ids]
    named = sum(picks).astype(bf16)
    earlier = one_hot(count((tok_rows, tok_rows), 0) < count((tok_rows, tok_rows), 1))
    before_it = jnp.dot(named, earlier, preferred_element_type=f32)
    ranks = [jnp.sum(pick * before_it, axis=0, keepdims=True) for pick in picks]
    group_count = count((4 * GROUPS, tok_rows), 0) * members
    in_group = ((ids[0] >= group_count) & (ids[0] < group_count + members)).astype(f32)
    group_before = jnp.dot(in_group.astype(bf16), earlier, preferred_element_type=f32)
    own_rank = jnp.sum(in_group * group_before, axis=0, keepdims=True)
    for g in range(GROUPS):
        inside = (count((group_cap, tok_rows), 0) == own_rank).astype(f32) * in_group[g : g + 1, :]
        gsel_ref[g] = inside.astype(bf16)

    def make_choice(g):
        slot_count = count((span, tok_rows), 0) + g * span
        hits = [one_hot(slot_count == value * capacity + rank) for value, rank in zip(ids, ranks)]
        choice_ref[g] = lax.dot_general(
            gsel_ref[g], sum(hits), (((1,), (1,)), ((), ())), preferred_element_type=f32
        ).astype(bf16)
        scales = sum(
            lax.dot_general(
                jnp.broadcast_to(weight_ref[pl.ds(k, 1), :].astype(f32), (16, tok_rows)).astype(bf16),
                hits[k], (((1,), (1,)), ((), ())), preferred_element_type=f32,
            )
            for k in range(topk)
        )
        scale_ref[g] = scales[:1]

    def route_back():
        table = back_route[...].reshape(experts, span).astype(bf16)
        lane = count((span, tok_rows), 0) - (seat * capacity).astype(f32)
        for k in range(topk):
            found = lax.dot_general(
                table, picks[k].astype(bf16), (((0,), (0,)), ((), ())), preferred_element_type=f32
            )
            chosen = jnp.where(lane == ranks[k], found, 0.0)
            route_out[pl.ds(k, 1), :] = jnp.sum(chosen, axis=0, keepdims=True).astype(bf16)

    down_acc[...] = jnp.zeros_like(down_acc)
    begun = set()
    grad_parts = [0, 0]

    def first_time(name):
        fresh = name not in begun
        begun.add(name)
        return fresh

    def send_scales():
        scale_in[0, seat] = scale_ref[group]
        for step in range(GROUPS):

            @pl.loop(0 if step else 1, members)
            def _(hop):
                scale_copy(step, hop).start()

    def run(token):
        name, step, i = token[:-2], int(token[-2]), int(token[-1])
        if halves < HALVES and name != "comp" and name != "grad":
            if i % HALVES:
                return
            i = i // HALVES
        if name == "far":
            packed[i, step, :, pl.ds(0, chunk_width(step, i))] = pack(step, i)
            if first_time("far"):
                pl.semaphore_wait(barrier, experts - 1 + splits - 1)
            far_copy(step, i).start()
        elif name == "spread":
            if first_time("spread"):
                for g in range(GROUPS):
                    make_choice(g)
                for other in range(1, GROUPS):
                    far_copy(other, 2 * halves).start()
            if step:
                arrive(step, i)
            else:
                spread(step, i, pack(step, i))
        elif name == "fwd":
            if first_time("fwd"):
                send_scales()
            forward(step, i)
        elif name == "comp":
            if first_time("comp"):
                for load in weight_loads:
                    load.wait()
            complete(step)
            compute(step)
            send_swaps(step)
        elif name == "red":
            if first_time("route%d" % step):
                route_home(step)
            reduce(step, i)
        elif name == "col":
            collect(step, i)
        elif step < 2:
            grads_in(grad_parts[0])
            grad_parts[0] += 1
            if grad_parts[0] == 2:
                for shift in range(1, splits):
                    small_square(shift).start()
        else:
            grads_down(grad_parts[1])
            grad_parts[1] += 1
            if grad_parts[1] == 2:
                down_square_out[...] = jnp.sum(down_acc[...].T, axis=0, keepdims=True)

    for load in input_loads:
        load.wait()
    for token in PLAN:
        run(token)

    for step in range(GROUPS):

        @pl.loop(0 if step else 1, members)
        def _(hop):
            route_copy(step, hop).wait_recv()

    route_back()
    for shift in range(1, splits):
        small_square(shift).wait_recv()
    value = square_mine[...]
    for shift in range(1, splits):
        value = value + peer_square[shift - 1]
    gate_square_out[...] = value[0]
    up_square_out[...] = value[1]
    selector = gsel_ref[...].reshape(GROUPS * group_cap, tok_rows)
    for b in range(halves):
        for step in range(1, GROUPS):
            home_copy(step, b).wait_recv()
        token_out[:, pl.ds(b * half_width, half_width)] = lax.dot_general(
            selector, back[b].reshape(GROUPS * group_cap, half_width), (((0,), (0,)), ((), ())),
            preferred_element_type=f32,
        ).astype(bf16)

    for step in range(GROUPS):
        if step:
            for b in range(halves):
                home_copy(step, b).wait_send()
            for i in range(2 * halves + 1):
                far_copy(step, i).wait_send()

        for i in chunks:
            each_hop(step, False, True, lambda hop: near_copy(step, hop, i).wait_send())
            if step == 0:
                mate_copy(i, mate_out).wait_send()

        @pl.loop(1, members)
        def _(hop):
            for b in range(halves):
                join_copy(step, b, hop).wait_send()

        def relays_sent(hop):
            for i in chunks:
                for shift in relays(step, i):
                    relay(step, hop, shift, i, col).wait_send()

        each_hop(step, True, False, relays_sent)

        @pl.loop(0, members)
        def _(hop):
            for shift in range(1, splits):
                for b in range(halves):
                    swap(step, b, hop, shift).wait_send()

        @pl.loop(0 if step else 1, members)
        def _(hop):
            scale_copy(step, hop).wait_send()
            route_copy(step, hop).wait_send()

        for shift in range(1, splits):
            small_route(step, shift).wait_send()
    for shift in range(1, splits):
        small_square(shift).wait_send()


def layer(ids, weights, tokens, cot, gate, up, down, experts, splits):
    members = experts // GROUPS
    topk, tok_rows = ids.shape
    model_width = tokens.shape[1]
    capacity = 2 * tok_rows * topk // experts
    span = members * capacity
    group_cap = span // topk
    hidden_width = gate.shape[1]
    width = model_width // splits
    halves = HALVES if experts * splits <= 64 else 1
    half_width, chunk, chunks = width // halves, model_width // halves, 2 * halves
    f32, bf16 = jnp.float32, jnp.bfloat16
    vmem = pl.BlockSpec(memory_space=pltpu.VMEM)
    hbm = pl.BlockSpec(memory_space=pltpu.HBM)
    tokens, cot, gate, up, down = (
        pltpu.with_memory_space_constraint(v, pltpu.HBM) for v in (tokens, cot, gate, up, down)
    )
    dma = pltpu.SemaphoreType.DMA
    shape = jax.ShapeDtypeStruct
    slots = (GROUPS, members, capacity)
    return pl.pallas_call(
        functools.partial(layer_kernel, experts, splits),
        out_shape=(
            shape((tok_rows, width), bf16),
            shape((topk, tok_rows), bf16),
            shape((model_width, hidden_width), bf16),
            shape((model_width, hidden_width), bf16),
            shape((1, model_width), f32),
            shape((1, model_width), f32),
            shape((hidden_width, model_width), bf16),
            shape((1, hidden_width), f32),
        ),
        in_specs=[vmem] * 2 + [hbm] * 5,
        out_specs=(vmem,) * 8,
        scratch_shapes=[
            pltpu.VMEM((tok_rows, model_width), bf16),
            pltpu.VMEM((tok_rows, model_width), bf16),
            pltpu.VMEM((GROUPS, group_cap, tok_rows), bf16),
            pltpu.VMEM((GROUPS, group_cap, span), bf16),
            pltpu.VMEM((GROUPS, 1, span), f32),
            pltpu.VMEM((experts, 1, span), f32),
            pltpu.VMEM((chunks, GROUPS, group_cap, chunk), bf16),
            pltpu.VMEM((chunks, GROUPS, group_cap, chunk), bf16),
            pltpu.VMEM((GROUPS, group_cap, span), bf16),
            pltpu.VMEM((chunks,) + slots + (chunk,), bf16),
            pltpu.VMEM((2,) + slots + (model_width,), bf16),
            pltpu.VMEM((GROUPS, members, 1, span), f32),
            pltpu.VMEM((model_width, 2 * hidden_width), bf16),
            pltpu.VMEM((hidden_width, model_width), bf16),
            pltpu.VMEM((GROUPS * span, 2 * hidden_width), bf16),
            pltpu.VMEM((GROUPS * span, hidden_width), bf16),
            pltpu.VMEM(slots + (model_width,), bf16),
            pltpu.VMEM((splits - 1, GROUPS, halves) + slots[1:] + (half_width,), bf16),
            pltpu.VMEM((GROUPS, halves) + slots[1:] + (half_width,), bf16),
            pltpu.VMEM((GROUPS, halves) + slots[1:] + (half_width,), bf16),
            pltpu.VMEM((GROUPS, halves, group_cap, half_width), bf16),
            pltpu.VMEM((halves, GROUPS, group_cap, half_width), bf16),
            pltpu.VMEM((GROUPS, 1, span), f32),
            pltpu.VMEM((splits - 1, GROUPS, 1, span), f32),
            pltpu.VMEM((GROUPS, 1, span), f32),
            pltpu.VMEM((2, 1, model_width), f32),
            pltpu.VMEM((splits - 1, 2, 1, model_width), f32),
            pltpu.VMEM((hidden_width, LANES), f32),
            dma((chunks + 1, GROUPS)), dma((chunks + 1, GROUPS)),
            dma((chunks, GROUPS, members)), dma((chunks, GROUPS, members)),
            dma((chunks, splits - 1, GROUPS, members)), dma((chunks, splits - 1, GROUPS, members)),
            dma((GROUPS, members)), dma((GROUPS, members)),
            dma((splits - 1, GROUPS, halves, members)), dma((splits - 1, GROUPS, halves, members)),
            dma((GROUPS, halves, members)), dma((GROUPS, halves, members)),
            dma((GROUPS, halves)), dma((GROUPS, halves)),
            dma((splits - 1, GROUPS)), dma((splits - 1, GROUPS)),
            dma((GROUPS, members)), dma((GROUPS, members)),
            dma((splits - 1,)), dma((splits - 1,)),
            dma((5,)),
        ],
        compiler_params=pltpu.CompilerParams(
            collective_id=0, has_side_effects=True, vmem_limit_bytes=40000 * 1024
        ),
    )(ids, weights, tokens, cot, gate, up, down)


def export_kernel(*refs):
    count = len(refs) // 2
    copies = [
        pltpu.make_async_copy(refs[n], refs[count + n], refs[-1].at[n]) for n in range(count)
    ]
    for copy in copies:
        copy.start()
    for copy in copies:
        copy.wait()


def export(arrays):
    return pl.pallas_call(
        export_kernel,
        out_shape=tuple(jax.ShapeDtypeStruct(a.shape, a.dtype) for a in arrays),
        in_specs=[pl.BlockSpec(memory_space=pltpu.VMEM)] * len(arrays),
        out_specs=(pl.BlockSpec(memory_space=pltpu.HBM),) * len(arrays),
        scratch_shapes=[pltpu.SemaphoreType.DMA((len(arrays),))],
        compiler_params=pltpu.CompilerParams(vmem_limit_bytes=8000 * 1024),
    )(*arrays)


def on_device(tokens, expert_ids, route_weights, cotangent, w_gate, w_up, w_down):
    experts = lax.axis_size("ep")
    splits = lax.axis_size("tp")
    results = layer(
        expert_ids.T, route_weights.T, tokens, cotangent, w_gate[0], w_up[0], w_down[0], experts, splits
    )
    token_grad, route_grad, grad_gate, grad_up, gate_square, up_square, grad_down, down_square = export(results)
    return (
        token_grad,
        route_grad.T,
        grad_gate[None],
        grad_up[None],
        grad_down[None],
        gate_square,
        up_square,
        down_square,
    )


def solution(mesh):
    return jax.shard_map(
        on_device,
        mesh=mesh,
        in_specs=(
            P("ep", None),
            P("ep", None),
            P("ep", None),
            P("ep", None),
            P("ep", None, "tp"),
            P("ep", None, "tp"),
            P("ep", "tp", None),
        ),
        out_specs=(
            P("ep", "tp"),
            P("ep", None),
            P("ep", None, "tp"),
            P("ep", None, "tp"),
            P("ep", "tp", None),
            P("ep", None),
            P("ep", None),
            P("ep", "tp"),
        ),
        check_vma=False,
    )
```

```python
import functools

import jax
import jax.numpy as jnp
from jax import lax
from jax.experimental import pallas as pl
from jax.experimental.layout import Layout, with_layout_constraint
from jax.experimental.pallas import tpu as pltpu
from jax.sharding import PartitionSpec as P

MESH = pl.DeviceIdType.MESH
LANES = 128
TILE = 256
GROUPS = 4
HALVES = 2
WHOLE = ((0, 1, 0, 0), (1, 1, 1, 1), (0, 0, 0, 0), (1, 1, 1, 1))
PLAN = (
    "far11", "far23", "spread03", "far22", "far21", "spread01", "spread00", "spread02", "fwd03",
    "far12", "spread23", "far20", "spread22", "far10", "fwd01", "far13", "far32", "fwd02", "spread11",
    "fwd22", "far30", "fwd23", "far33", "spread21", "spread20", "fwd00", "spread12", "spread10",
    "fwd20", "fwd21", "fwd11", "spread13", "comp00", "spread32", "comp20", "fwd13", "far31",
    "fwd32", "spread30", "fwd10", "spread33", "fwd12", "comp10", "spread31", "red01", "fwd33",
    "fwd30", "red20", "red21", "fwd31", "comp30", "red10", "grad10", "red00", "col20", "red11",
    "col10", "col21", "red30", "grad30", "red31", "col00", "col30", "col31", "col11", "col01",
    "grad20", "grad00",
)


def greet(experts, splits, me, col):
    barrier = pltpu.get_barrier_semaphore()

    @pl.loop(1, experts)
    def _(off):
        pl.semaphore_signal(
            barrier, inc=1, device_id={"ep": lax.rem(me + off, experts), "tp": col}, device_id_type=MESH
        )

    for shift in range(1, splits):
        pl.semaphore_signal(
            barrier, inc=1, device_id={"ep": me, "tp": lax.rem(col + shift, splits)}, device_id_type=MESH
        )
    return barrier


def remote(src, dst, send, recv, ep, tp):
    return pltpu.make_async_remote_copy(
        src_ref=src,
        dst_ref=dst,
        send_sem=send,
        recv_sem=recv,
        device_id={"ep": ep, "tp": tp},
        device_id_type=MESH,
    )


def partner(group, step):
    if step == 0:
        return group
    if step == 1:
        return group + 1 - 2 * lax.rem(group, 2)
    if step == 2:
        return lax.rem(group + 2, GROUPS)
    return GROUPS - 1 - group


def layer_kernel(
    experts, splits,
    ids_hbm, weight_hbm, tokens_hbm, cot_hbm, gate_hbm, up_hbm, down_hbm,
    token_out, route_out, gate_out, up_out, gate_square_out, up_square_out, down_out, down_square_out,
    ids_ref, weight_ref, tokens_ref, cot_ref, gsel_ref, choice_ref, scale_ref, back_route, packed, landed, landed_choice, stage, rows, scale_in, wide, down, cots, weighted,
    part, peer_part, total, gathered, finished, back, route_mine, peer_route, route_total,
    square_mine, peer_square, down_acc,
    far_send, far_recv, near_send, near_recv, relay_send, relay_recv, scale_send, scale_recv,
    swap_send, swap_recv, join_send, join_recv, home_send, home_recv, small_send, small_recv,
    route_send, route_recv, square_send, square_recv, local,
):
    me = lax.axis_index("ep")
    col = lax.axis_index("tp")
    members = experts // GROUPS
    group = me // members
    seat = lax.rem(me, members)
    model_width = tokens_ref.shape[1]
    capacity = rows.shape[3]
    span = members * capacity
    hidden_width = down.shape[0]
    width = model_width // splits
    f32, bf16 = jnp.float32, jnp.bfloat16
    halves = peer_part.shape[2]
    half_width = width // halves
    chunk = model_width // halves
    chunks = range(2 * halves)
    places = [partner(group, step) for step in range(GROUPS)]
    barrier = greet(experts, splits, me, col)
    inputs = (tokens_ref, cot_ref)

    weight_loads = (
        pltpu.make_async_copy(gate_hbm, wide.at[:, pl.ds(0, hidden_width)], local.at[0]),
        pltpu.make_async_copy(up_hbm, wide.at[:, pl.ds(hidden_width, hidden_width)], local.at[1]),
        pltpu.make_async_copy(down_hbm, down, local.at[2]),
    )
    input_loads = (
        pltpu.make_async_copy(tokens_hbm, tokens_ref, local.at[3]),
        pltpu.make_async_copy(cot_hbm, cot_ref, local.at[4]),
    )
    route_loads = (
        pltpu.make_async_copy(ids_hbm, ids_ref, local.at[5]),
        pltpu.make_async_copy(weight_hbm, weight_ref, local.at[6]),
    )
    for load in route_loads + input_loads + weight_loads:
        load.start()

    def whole(step, i):
        return WHOLE[step][i * HALVES // halves]

    def chunk_width(step, i):
        return chunk if whole(step, i) else chunk // splits

    def window(step, i):
        base = i % halves * chunk
        if whole(step, i):
            return pl.ds(base, chunk)
        return relay_part(step, i, col)

    def relay_part(step, i, which):
        cut = chunk // splits
        return pl.ds(pl.multiple_of(i % halves * chunk + which * cut, LANES), cut)

    def around(hop):
        return lax.rem(seat + hop, members)

    def before(hop):
        return lax.rem(seat + members - hop, members)

    def far_copy(step, i):
        if i == 2 * halves:
            source, target = choice_ref.at[places[step]], landed_choice.at[step]
        else:
            cols = pl.ds(0, chunk_width(step, i))
            source, target = packed.at[i, step, :, cols], landed.at[i, step, :, cols]
        return remote(
            source, target, far_send.at[i, step], far_recv.at[i, step],
            places[step] * members + seat, col,
        )

    def scale_copy(step, hop):
        there = places[step] * members + around(hop)
        return remote(
            scale_ref.at[places[step]], scale_in.at[step, seat],
            scale_send.at[step, hop], scale_recv.at[step, hop], there, col,
        )

    mate = seat + 1 - 2 * lax.rem(seat, 2)
    chip = seat - lax.rem(seat, 2)

    def mate_copy(i, hop):
        return remote(
            stage.at[i, 0, mate], rows.at[i // halves, 0, seat, :, pl.ds(i % halves * chunk, chunk)], near_send.at[i, 0, hop], near_recv.at[i, 0, hop],
            group * members + mate, col,
        )

    mate_out = lax.rem(mate - seat + members, members)
    mate_in = lax.rem(seat - mate + members, members)

    def each_hop(step, own, outgoing, act):
        if step:
            first = 0 if own else 1

            @pl.loop(first, members)
            def _(hop):
                act(hop)
        else:

            @pl.loop(2, members)
            def _(turn):
                other = lax.rem(chip + turn, members)
                gap = other - seat if outgoing else seat - other
                act(lax.rem(gap + members, members))

    def near_copy(step, hop, i):
        size = chunk_width(step, i)
        start = 0 if step or whole(step, i) else pl.multiple_of(col * size, LANES)
        return remote(
            stage.at[i, step, around(hop), :, pl.ds(start, size)],
            rows.at[i // halves, step, seat, :, window(step, i)],
            near_send.at[i, step, hop], near_recv.at[i, step, hop], group * members + around(hop), col,
        )

    def relay(step, hop, shift, i, which):
        block = rows.at[i // halves, step, before(hop), :, relay_part(step, i, which)]
        return remote(
            block, block, relay_send.at[i, shift - 1, step, hop], relay_recv.at[i, shift - 1, step, hop],
            me, lax.rem(col + shift, splits),
        )

    def swap(step, b, shift):
        peer = lax.rem(col + shift, splits)
        theirs = pl.ds(pl.multiple_of(peer * width + b * half_width, LANES), half_width)
        return remote(
            part.at[step, :, :, theirs], peer_part.at[shift - 1, step, b],
            swap_send.at[shift - 1, step, b], swap_recv.at[shift - 1, step, b], me, peer,
        )

    def small_route(step, shift):
        return remote(
            route_mine.at[step], peer_route.at[shift - 1, step],
            small_send.at[shift - 1, step], small_recv.at[shift - 1, step],
            me, lax.rem(col + shift, splits),
        )

    def small_square(shift):
        return remote(
            square_mine, peer_square.at[shift - 1], square_send.at[shift - 1], square_recv.at[shift - 1],
            me, lax.rem(col + shift, splits),
        )

    def join_copy(step, b, hop):
        return remote(
            total.at[step, b, hop], gathered.at[step, b, seat],
            join_send.at[step, b, hop], join_recv.at[step, b, hop], group * members + around(hop), col,
        )

    def home_copy(step, b):
        return remote(
            finished.at[step, b], back.at[b, group], home_send.at[step, b], home_recv.at[step, b],
            places[step] * members + seat, col,
        )

    def route_copy(step, hop):
        there = places[step] * members + around(hop)
        return remote(
            route_total.at[step], back_route.at[me], route_send.at[step, hop], route_recv.at[step, hop],
            there, col,
        )

    def pack(step, i):
        cols = window(step, i) if step else pl.ds(i % halves * chunk, chunk)
        source = inputs[i // halves][:, cols]
        return jnp.dot(gsel_ref[places[step]], source, preferred_element_type=f32).astype(bf16)

    def spread(step, i, block):
        choice = landed_choice[step] if step else choice_ref[group]
        value = lax.dot_general(choice, block, (((0,), (0,)), ((), ())), preferred_element_type=f32)
        wide_cut = block.shape[1]
        stage[i, step, :, :, pl.ds(0, wide_cut)] = value.astype(bf16).reshape(members, capacity, wide_cut)
        if step == 0:
            mate_copy(i, mate_out).start()
        each_hop(step, False, True, lambda hop: near_copy(step, hop, i).start())

        cols = window(step, i) if step else pl.ds(i % halves * chunk, chunk)
        rows[i // halves, step, seat, :, cols] = stage[i, step, seat, :, pl.ds(0, wide_cut)]
        if step:
            for shift in relays(step, i):
                relay(step, 0, shift, i, col).start()

    def relays(step, i):
        return () if whole(step, i) else range(1, splits)

    choices = set()

    def arrive(step, i):
        if step not in choices:
            choices.add(step)
            far_copy(step, 2 * halves).wait_recv()
        far_copy(step, i).wait_recv()
        spread(step, i, landed[i, step, :, pl.ds(0, chunk_width(step, i))])

    def forward(step, i):
        def pass_on(hop):
            near_copy(step, hop, i).wait_recv()
            for shift in relays(step, i):
                relay(step, hop, shift, i, col).start()

        each_hop(step, False, False, pass_on)
        if step == 0:
            mate_copy(i, mate_in).wait_recv()

    def complete(step):
        def landed_all(hop):
            for i in chunks:
                for shift in relays(step, i):
                    relay(step, hop, shift, i, lax.rem(col + splits - shift, splits)).wait_recv()

        each_hop(step, True, False, landed_all)

        @pl.loop(0 if step else 1, members)
        def _(hop):
            scale_copy(step, hop).wait_recv()

    def compute(step):
        slot_rows = rows[0, step].reshape(span, model_width)
        slot_cot = rows[1, step].reshape(span, model_width)
        pre = jnp.dot(slot_rows, wide[...], preferred_element_type=f32)
        gate_pre, up_pre = pre[:, :hidden_width], pre[:, hidden_width:]
        hidden_back = lax.dot_general(
            slot_cot, down[...], (((1,), (1,)), ((), ())), preferred_element_type=f32
        )
        spread_scale = jnp.broadcast_to(scale_in[step], (members, capacity, span))
        lane = lax.broadcasted_iota(jnp.int32, (members, capacity, span), 2)
        slot = lax.broadcasted_iota(jnp.int32, (members, capacity, span), 1) + seat * capacity
        scale = jnp.sum(jnp.where(lane == slot, spread_scale, 0.0), axis=2, keepdims=True)
        scale = scale.reshape(span, 1)
        gate_sig = jax.nn.sigmoid(gate_pre)
        activated = gate_pre * gate_sig
        hidden = activated * up_pre
        route = hidden * hidden_back
        folded = route[:, :LANES]
        for start in range(LANES, hidden_width, LANES):
            folded = folded + route[:, start : start + LANES]
        route_mine[step] = jnp.sum(folded.T, axis=0, keepdims=True)
        hidden_cot = scale * hidden_back
        up_cot = (hidden_cot * activated).astype(bf16)
        gate_cot = (hidden_cot * up_pre * gate_sig * (1.0 + gate_pre * (1.0 - gate_sig))).astype(bf16)
        slots = pl.ds(step * span, span)
        cots[slots, pl.ds(0, hidden_width)] = gate_cot
        cots[slots, pl.ds(hidden_width, hidden_width)] = up_cot
        weighted[slots, :] = (scale * hidden).astype(bf16)
        both = cots[slots, :]

        @pl.loop(0, model_width // (2 * TILE))
        def _(tile):
            cols = pl.ds(pl.multiple_of(tile * 2 * TILE, LANES), 2 * TILE)
            term = lax.dot_general(
                both, wide[cols, :], (((1,), (1,)), ((), ())), preferred_element_type=f32
            )
            part[step, :, :, cols] = term.astype(bf16).reshape(members, capacity, 2 * TILE)

        for shift in range(1, splits):
            small_route(step, shift).start()

    def send_swaps(step):
        for b in range(halves):
            for shift in range(1, splits):
                swap(step, b, shift).start()

    def route_home(step):
        value = route_mine[step]
        for shift in range(1, splits):
            small_route(step, shift).wait_recv()
            value = value + peer_route[shift - 1, step]
        route_total[step] = value
        if step == 0:
            back_route[me] = value

        @pl.loop(0 if step else 1, members)
        def _(hop):
            route_copy(step, hop).start()

    def block_total(step, b, hop):
        source = around(hop)
        mine = pl.ds(pl.multiple_of(col * width + b * half_width, LANES), half_width)
        value = part[step, source, :, mine].astype(f32)
        for shift in range(1, splits):
            value = value + peer_part[shift - 1, step, b, source].astype(f32)
        return value.astype(bf16)

    def reduce(step, b):
        for shift in range(1, splits):
            swap(step, b, shift).wait_recv()

        @pl.loop(1, members)
        def _(hop):
            total[step, b, hop] = block_total(step, b, hop)
            join_copy(step, b, hop).start()

        gathered[step, b, seat] = block_total(step, b, 0)

    def collect(step, b):
        @pl.loop(1, members)
        def _(hop):
            join_copy(step, b, hop).wait_recv()

        pairs = gathered[step, b].reshape(span, half_width)
        choice = landed_choice[step] if step else choice_ref[group]
        summed = jnp.dot(choice, pairs, preferred_element_type=f32).astype(bf16)
        if step:
            finished[step, b] = summed
            home_copy(step, b).start()
        else:
            back[b, group] = summed

    def lane_sums(value):
        folded = value[:, :LANES]
        for start in range(LANES, value.shape[1], LANES):
            folded = folded + value[:, start : start + LANES]
        return folded

    def grads_in(first):
        tiles = model_width // TILE // 2

        @pl.loop(first * tiles, (first + 1) * tiles)
        def _(tile):
            cols = pl.ds(pl.multiple_of(tile * TILE, LANES), TILE)
            left = rows[0, :, :, :, cols].reshape(GROUPS * span, TILE)
            grad = lax.dot_general(
                left, cots[...], (((0,), (0,)), ((), ())), preferred_element_type=f32
            ).astype(bf16)
            for n, out in enumerate((gate_out, up_out)):
                value = grad[:, n * hidden_width : (n + 1) * hidden_width]
                out[cols, :] = value
                square = lane_sums(jnp.square(value.astype(f32)))
                square_mine[n, :, cols] = jnp.sum(square.T, axis=0, keepdims=True)

    def grads_down(first):
        tiles = model_width // TILE // 4

        @pl.loop(first * tiles, (first + 1) * tiles)
        def _(tile):
            cols = pl.ds(pl.multiple_of(tile * 2 * TILE, LANES), 2 * TILE)
            right = rows[1, :, :, :, cols].reshape(GROUPS * span, 2 * TILE)
            grad = lax.dot_general(
                weighted[...], right, (((0,), (0,)), ((), ())), preferred_element_type=f32
            ).astype(bf16)
            down_out[:, cols] = grad
            down_acc[...] += lane_sums(jnp.square(grad.astype(f32)))

    for load in route_loads:
        load.wait()
    topk, tok_rows = ids_ref.shape
    group_cap = gsel_ref.shape[1]

    def count(shape, axis):
        return lax.broadcasted_iota(jnp.int32, shape, axis).astype(f32)

    def one_hot(mask):
        return mask.astype(f32).astype(bf16)

    ids = [ids_ref[pl.ds(k, 1), :].astype(f32) for k in range(topk)]
    expert_count = count((experts, tok_rows), 0)
    picks = [(expert_count == value).astype(f32) for value in ids]
    named = sum(picks).astype(bf16)
    earlier = one_hot(count((tok_rows, tok_rows), 0) < count((tok_rows, tok_rows), 1))
    before_it = jnp.dot(named, earlier, preferred_element_type=f32)
    ranks = [jnp.sum(pick * before_it, axis=0, keepdims=True) for pick in picks]
    group_count = count((4 * GROUPS, tok_rows), 0) * members
    in_group = ((ids[0] >= group_count) & (ids[0] < group_count + members)).astype(f32)
    group_before = jnp.dot(in_group.astype(bf16), earlier, preferred_element_type=f32)
    own_rank = jnp.sum(in_group * group_before, axis=0, keepdims=True)
    for g in range(GROUPS):
        inside = (count((group_cap, tok_rows), 0) == own_rank).astype(f32) * in_group[g : g + 1, :]
        gsel_ref[g] = inside.astype(bf16)

    def make_choice(g):
        slot_count = count((span, tok_rows), 0) + g * span
        hits = [one_hot(slot_count == value * capacity + rank) for value, rank in zip(ids, ranks)]
        choice_ref[g] = lax.dot_general(
            gsel_ref[g], sum(hits), (((1,), (1,)), ((), ())), preferred_element_type=f32
        ).astype(bf16)
        scales = sum(
            lax.dot_general(
                jnp.broadcast_to(weight_ref[pl.ds(k, 1), :].astype(f32), (16, tok_rows)).astype(bf16),
                hits[k], (((1,), (1,)), ((), ())), preferred_element_type=f32,
            )
            for k in range(topk)
        )
        scale_ref[g] = scales[:1]

    def route_back():
        table = back_route[...].reshape(experts, span).astype(bf16)
        lane = count((span, tok_rows), 0) - (seat * capacity).astype(f32)
        for k in range(topk):
            found = lax.dot_general(
                table, picks[k].astype(bf16), (((0,), (0,)), ((), ())), preferred_element_type=f32
            )
            chosen = jnp.where(lane == ranks[k], found, 0.0)
            route_out[pl.ds(k, 1), :] = jnp.sum(chosen, axis=0, keepdims=True).astype(bf16)

    down_acc[...] = jnp.zeros_like(down_acc)
    begun = set()
    grad_parts = [0, 0]

    def first_time(name):
        fresh = name not in begun
        begun.add(name)
        return fresh

    def send_scales():
        scale_in[0, seat] = scale_ref[group]
        for step in range(GROUPS):

            @pl.loop(0 if step else 1, members)
            def _(hop):
                scale_copy(step, hop).start()

    def run(token):
        name, step, i = token[:-2], int(token[-2]), int(token[-1])
        if halves < HALVES and name != "comp" and name != "grad":
            if i % HALVES:
                return
            i = i // HALVES
        if name == "far":
            packed[i, step, :, pl.ds(0, chunk_width(step, i))] = pack(step, i)
            if first_time("far"):
                pl.semaphore_wait(barrier, experts - 1 + splits - 1)
            far_copy(step, i).start()
        elif name == "spread":
            if first_time("spread"):
                for g in range(GROUPS):
                    make_choice(g)
                for other in range(1, GROUPS):
                    far_copy(other, 2 * halves).start()
            if step:
                arrive(step, i)
            else:
                spread(step, i, pack(step, i))
        elif name == "fwd":
            if first_time("fwd"):
                send_scales()
            forward(step, i)
        elif name == "comp":
            if first_time("comp"):
                for load in weight_loads:
                    load.wait()
            complete(step)
            compute(step)
            send_swaps(step)
        elif name == "red":
            if first_time("route%d" % step):
                route_home(step)
            reduce(step, i)
        elif name == "col":
            collect(step, i)
        elif step < 2:
            grads_in(grad_parts[0])
            grad_parts[0] += 1
            if grad_parts[0] == 2:
                for shift in range(1, splits):
                    small_square(shift).start()
        else:
            grads_down(grad_parts[1])
            grad_parts[1] += 1
            if grad_parts[1] == 2:
                down_square_out[...] = jnp.sum(down_acc[...].T, axis=0, keepdims=True)

    for load in input_loads:
        load.wait()
    for token in PLAN:
        run(token)

    for step in range(GROUPS):

        @pl.loop(0 if step else 1, members)
        def _(hop):
            route_copy(step, hop).wait_recv()

    route_back()
    for shift in range(1, splits):
        small_square(shift).wait_recv()
    value = square_mine[...]
    for shift in range(1, splits):
        value = value + peer_square[shift - 1]
    gate_square_out[...] = value[0]
    up_square_out[...] = value[1]
    selector = gsel_ref[...].reshape(GROUPS * group_cap, tok_rows)
    for b in range(halves):
        for step in range(1, GROUPS):
            home_copy(step, b).wait_recv()
        token_out[:, pl.ds(b * half_width, half_width)] = lax.dot_general(
            selector, back[b].reshape(GROUPS * group_cap, half_width), (((0,), (0,)), ((), ())),
            preferred_element_type=f32,
        ).astype(bf16)

    for step in range(GROUPS):
        if step:
            for b in range(halves):
                home_copy(step, b).wait_send()
            for i in range(2 * halves + 1):
                far_copy(step, i).wait_send()

        for i in chunks:
            each_hop(step, False, True, lambda hop: near_copy(step, hop, i).wait_send())
            if step == 0:
                mate_copy(i, mate_out).wait_send()

        @pl.loop(1, members)
        def _(hop):
            for b in range(halves):
                join_copy(step, b, hop).wait_send()

        def relays_sent(hop):
            for i in chunks:
                for shift in relays(step, i):
                    relay(step, hop, shift, i, col).wait_send()

        each_hop(step, True, False, relays_sent)

        for shift in range(1, splits):
            for b in range(halves):
                swap(step, b, shift).wait_send()

        @pl.loop(0 if step else 1, members)
        def _(hop):
            scale_copy(step, hop).wait_send()
            route_copy(step, hop).wait_send()

        for shift in range(1, splits):
            small_route(step, shift).wait_send()
    for shift in range(1, splits):
        small_square(shift).wait_send()


def layer(ids, weights, tokens, cot, gate, up, down, experts, splits):
    members = experts // GROUPS
    topk, tok_rows = ids.shape
    model_width = tokens.shape[1]
    capacity = 2 * tok_rows * topk // experts
    span = members * capacity
    group_cap = span // topk
    hidden_width = gate.shape[1]
    width = model_width // splits
    halves = HALVES if experts * splits <= 64 else 1
    half_width, chunk, chunks = width // halves, model_width // halves, 2 * halves
    f32, bf16 = jnp.float32, jnp.bfloat16
    vmem = pl.BlockSpec(memory_space=pltpu.VMEM)
    hbm = pl.BlockSpec(memory_space=pltpu.HBM)
    ids, weights, tokens, cot, gate, up, down = (
        pltpu.with_memory_space_constraint(v, pltpu.HBM)
        for v in (ids, weights, tokens, cot, gate, up, down)
    )
    dma = pltpu.SemaphoreType.DMA
    shape = jax.ShapeDtypeStruct
    slots = (GROUPS, members, capacity)
    return pl.pallas_call(
        functools.partial(layer_kernel, experts, splits),
        out_shape=(
            shape((tok_rows, width), bf16),
            shape((topk, tok_rows), bf16),
            shape((model_width, hidden_width), bf16),
            shape((model_width, hidden_width), bf16),
            shape((1, model_width), f32),
            shape((1, model_width), f32),
            shape((hidden_width, model_width), bf16),
            shape((1, hidden_width), f32),
        ),
        in_specs=[hbm] * 7,
        out_specs=(vmem,) * 8,
        scratch_shapes=[
            pltpu.VMEM((topk, tok_rows), jnp.int32),
            pltpu.VMEM((topk, tok_rows), bf16),
            pltpu.VMEM((tok_rows, model_width), bf16),
            pltpu.VMEM((tok_rows, model_width), bf16),
            pltpu.VMEM((GROUPS, group_cap, tok_rows), bf16),
            pltpu.VMEM((GROUPS, group_cap, span), bf16),
            pltpu.VMEM((GROUPS, 1, span), f32),
            pltpu.VMEM((experts, 1, span), f32),
            pltpu.VMEM((chunks, GROUPS, group_cap, chunk), bf16),
            pltpu.VMEM((chunks, GROUPS, group_cap, chunk), bf16),
            pltpu.VMEM((GROUPS, group_cap, span), bf16),
            pltpu.VMEM((chunks,) + slots + (chunk,), bf16),
            pltpu.VMEM((2,) + slots + (model_width,), bf16),
            pltpu.VMEM((GROUPS, members, 1, span), f32),
            pltpu.VMEM((model_width, 2 * hidden_width), bf16),
            pltpu.VMEM((hidden_width, model_width), bf16),
            pltpu.VMEM((GROUPS * span, 2 * hidden_width), bf16),
            pltpu.VMEM((GROUPS * span, hidden_width), bf16),
            pltpu.VMEM(slots + (model_width,), bf16),
            pltpu.VMEM((splits - 1, GROUPS, halves) + slots[1:] + (half_width,), bf16),
            pltpu.VMEM((GROUPS, halves) + slots[1:] + (half_width,), bf16),
            pltpu.VMEM((GROUPS, halves) + slots[1:] + (half_width,), bf16),
            pltpu.VMEM((GROUPS, halves, group_cap, half_width), bf16),
            pltpu.VMEM((halves, GROUPS, group_cap, half_width), bf16),
            pltpu.VMEM((GROUPS, 1, span), f32),
            pltpu.VMEM((splits - 1, GROUPS, 1, span), f32),
            pltpu.VMEM((GROUPS, 1, span), f32),
            pltpu.VMEM((2, 1, model_width), f32),
            pltpu.VMEM((splits - 1, 2, 1, model_width), f32),
            pltpu.VMEM((hidden_width, LANES), f32),
            dma((chunks + 1, GROUPS)), dma((chunks + 1, GROUPS)),
            dma((chunks, GROUPS, members)), dma((chunks, GROUPS, members)),
            dma((chunks, splits - 1, GROUPS, members)), dma((chunks, splits - 1, GROUPS, members)),
            dma((GROUPS, members)), dma((GROUPS, members)),
            dma((splits - 1, GROUPS, halves)), dma((splits - 1, GROUPS, halves)),
            dma((GROUPS, halves, members)), dma((GROUPS, halves, members)),
            dma((GROUPS, halves)), dma((GROUPS, halves)),
            dma((splits - 1, GROUPS)), dma((splits - 1, GROUPS)),
            dma((GROUPS, members)), dma((GROUPS, members)),
            dma((splits - 1,)), dma((splits - 1,)),
            dma((7,)),
        ],
        compiler_params=pltpu.CompilerParams(
            collective_id=0, has_side_effects=True, vmem_limit_bytes=40000 * 1024
        ),
    )(ids, weights, tokens, cot, gate, up, down)


def export_kernel(*refs):
    count = len(refs) // 2
    copies = [
        pltpu.make_async_copy(refs[n], refs[count + n], refs[-1].at[n]) for n in range(count)
    ]
    for copy in copies:
        copy.start()
    for copy in copies:
        copy.wait()


def export(arrays):
    return pl.pallas_call(
        export_kernel,
        out_shape=tuple(jax.ShapeDtypeStruct(a.shape, a.dtype) for a in arrays),
        in_specs=[pl.BlockSpec(memory_space=pltpu.VMEM)] * len(arrays),
        out_specs=(pl.BlockSpec(memory_space=pltpu.HBM),) * len(arrays),
        scratch_shapes=[pltpu.SemaphoreType.DMA((len(arrays),))],
        compiler_params=pltpu.CompilerParams(vmem_limit_bytes=8000 * 1024),
    )(*arrays)


def on_device(tokens, expert_ids, route_weights, cotangent, w_gate, w_up, w_down):
    experts = lax.axis_size("ep")
    splits = lax.axis_size("tp")
    results = layer(
        expert_ids.T, route_weights.T, tokens, cotangent, w_gate[0], w_up[0], w_down[0], experts, splits
    )
    token_grad, route_grad, grad_gate, grad_up, gate_square, up_square, grad_down, down_square = export(results)
    return (
        token_grad,
        route_grad.T,
        grad_gate[None],
        grad_up[None],
        grad_down[None],
        gate_square,
        up_square,
        down_square,
    )


def solution(mesh):
    return jax.shard_map(
        on_device,
        mesh=mesh,
        in_specs=(
            P("ep", None),
            P("ep", None),
            P("ep", None),
            P("ep", None),
            P("ep", None, "tp"),
            P("ep", None, "tp"),
            P("ep", "tp", None),
        ),
        out_specs=(
            P("ep", "tp"),
            P("ep", None),
            P("ep", None, "tp"),
            P("ep", None, "tp"),
            P("ep", "tp", None),
            P("ep", None),
            P("ep", None),
            P("ep", "tp"),
        ),
        check_vma=False,
    )
```

```python
import functools

import jax
import jax.numpy as jnp
from jax import lax
from jax.experimental import pallas as pl
from jax.experimental.layout import Layout, with_layout_constraint
from jax.experimental.pallas import tpu as pltpu
from jax.sharding import PartitionSpec as P

MESH = pl.DeviceIdType.MESH
LANES = 128
TILE = 256
GROUPS = 4
HALVES = 2
WHOLE = ((0, 0, 0, 0), (1, 1, 1, 1), (0, 0, 0, 0), (1, 1, 1, 1))
PLAN = (
    "far11", "far23", "spread03", "far22", "far21", "spread01", "spread00", "spread02", "fwd03",
    "far12", "spread23", "far20", "spread22", "far10", "fwd01", "far13", "far32", "fwd02", "spread11",
    "fwd22", "far30", "fwd23", "far33", "spread21", "spread20", "fwd00", "spread12", "spread10",
    "fwd20", "fwd21", "fwd11", "spread13", "comp00", "spread32", "comp20", "fwd13", "far31",
    "fwd32", "spread30", "fwd10", "spread33", "fwd12", "comp10", "spread31", "red01", "fwd33",
    "fwd30", "red20", "red21", "fwd31", "comp30", "red10", "grad10", "red00", "col20", "red11",
    "col10", "col21", "red30", "grad30", "red31", "col00", "col30", "col31", "col11", "col01",
    "grad20", "grad00",
)


def greet(experts, splits, me, col):
    barrier = pltpu.get_barrier_semaphore()

    @pl.loop(1, experts)
    def _(off):
        pl.semaphore_signal(
            barrier, inc=1, device_id={"ep": lax.rem(me + off, experts), "tp": col}, device_id_type=MESH
        )

    for shift in range(1, splits):
        pl.semaphore_signal(
            barrier, inc=1, device_id={"ep": me, "tp": lax.rem(col + shift, splits)}, device_id_type=MESH
        )
    return barrier


def remote(src, dst, send, recv, ep, tp):
    return pltpu.make_async_remote_copy(
        src_ref=src,
        dst_ref=dst,
        send_sem=send,
        recv_sem=recv,
        device_id={"ep": ep, "tp": tp},
        device_id_type=MESH,
    )


def partner(group, step):
    if step == 0:
        return group
    if step == 1:
        return group + 1 - 2 * lax.rem(group, 2)
    if step == 2:
        return lax.rem(group + 2, GROUPS)
    return GROUPS - 1 - group


def layer_kernel(
    experts, splits,
    ids_hbm, weight_hbm, tokens_hbm, cot_hbm, gate_hbm, up_hbm, down_hbm,
    token_out, route_out, gate_out, up_out, gate_square_out, up_square_out, down_out, down_square_out,
    ids_ref, weight_ref, tokens_ref, cot_ref, gsel_ref, choice_ref, scale_ref, back_route, packed, landed, landed_choice, stage, rows, scale_in, wide, down, cots, weighted,
    part, peer_part, total, gathered, finished, back, route_mine, peer_route, route_total,
    square_mine, peer_square, down_acc,
    far_send, far_recv, near_send, near_recv, relay_send, relay_recv, scale_send, scale_recv,
    swap_send, swap_recv, join_send, join_recv, home_send, home_recv, small_send, small_recv,
    route_send, route_recv, square_send, square_recv, local,
):
    me = lax.axis_index("ep")
    col = lax.axis_index("tp")
    members = experts // GROUPS
    group = me // members
    seat = lax.rem(me, members)
    model_width = tokens_ref.shape[1]
    capacity = rows.shape[3]
    span = members * capacity
    hidden_width = down.shape[0]
    width = model_width // splits
    f32, bf16 = jnp.float32, jnp.bfloat16
    halves = peer_part.shape[2]
    half_width = width // halves
    chunk = model_width // halves
    chunks = range(2 * halves)
    places = [partner(group, step) for step in range(GROUPS)]
    barrier = greet(experts, splits, me, col)
    inputs = (tokens_ref, cot_ref)

    weight_loads = (
        pltpu.make_async_copy(gate_hbm, wide.at[:, pl.ds(0, hidden_width)], local.at[0]),
        pltpu.make_async_copy(up_hbm, wide.at[:, pl.ds(hidden_width, hidden_width)], local.at[1]),
        pltpu.make_async_copy(down_hbm, down, local.at[2]),
    )
    input_loads = (
        pltpu.make_async_copy(tokens_hbm, tokens_ref, local.at[3]),
        pltpu.make_async_copy(cot_hbm, cot_ref, local.at[4]),
    )
    route_loads = (
        pltpu.make_async_copy(ids_hbm, ids_ref, local.at[5]),
        pltpu.make_async_copy(weight_hbm, weight_ref, local.at[6]),
    )
    for load in route_loads + input_loads + weight_loads:
        load.start()

    def whole(step, i):
        return WHOLE[step][i * HALVES // halves]

    def chunk_width(step, i):
        return chunk if whole(step, i) else chunk // splits

    def window(step, i):
        base = i % halves * chunk
        if whole(step, i):
            return pl.ds(base, chunk)
        return relay_part(step, i, col)

    def relay_part(step, i, which):
        cut = chunk // splits
        return pl.ds(pl.multiple_of(i % halves * chunk + which * cut, LANES), cut)

    def around(hop):
        return lax.rem(seat + hop, members)

    def before(hop):
        return lax.rem(seat + members - hop, members)

    def far_copy(step, i):
        if i == 2 * halves:
            source, target = choice_ref.at[places[step]], landed_choice.at[step]
        else:
            cols = pl.ds(0, chunk_width(step, i))
            source, target = packed.at[i, step, :, cols], landed.at[i, step, :, cols]
        return remote(
            source, target, far_send.at[i, step], far_recv.at[i, step],
            places[step] * members + seat, col,
        )

    def scale_copy(step, hop):
        there = places[step] * members + around(hop)
        return remote(
            scale_ref.at[places[step]], scale_in.at[step, seat],
            scale_send.at[step, hop], scale_recv.at[step, hop], there, col,
        )

    mate = seat + 1 - 2 * lax.rem(seat, 2)
    chip = seat - lax.rem(seat, 2)

    def mate_copy(i, hop):
        return remote(
            stage.at[i, 0, mate], rows.at[i // halves, 0, seat, :, pl.ds(i % halves * chunk, chunk)], near_send.at[i, 0, hop], near_recv.at[i, 0, hop],
            group * members + mate, col,
        )

    mate_out = lax.rem(mate - seat + members, members)
    mate_in = lax.rem(seat - mate + members, members)

    def each_hop(step, own, outgoing, act):
        if step:
            first = 0 if own else 1

            @pl.loop(first, members)
            def _(hop):
                act(hop)
        else:

            @pl.loop(2, members)
            def _(turn):
                other = lax.rem(chip + turn, members)
                gap = other - seat if outgoing else seat - other
                act(lax.rem(gap + members, members))

    def near_copy(step, hop, i):
        size = chunk_width(step, i)
        start = 0 if step or whole(step, i) else pl.multiple_of(col * size, LANES)
        return remote(
            stage.at[i, step, around(hop), :, pl.ds(start, size)],
            rows.at[i // halves, step, seat, :, window(step, i)],
            near_send.at[i, step, hop], near_recv.at[i, step, hop], group * members + around(hop), col,
        )

    def relay(step, hop, shift, i, which):
        block = rows.at[i // halves, step, before(hop), :, relay_part(step, i, which)]
        return remote(
            block, block, relay_send.at[i, shift - 1, step, hop], relay_recv.at[i, shift - 1, step, hop],
            me, lax.rem(col + shift, splits),
        )

    def swap(step, b, shift):
        peer = lax.rem(col + shift, splits)
        theirs = pl.ds(pl.multiple_of(peer * width + b * half_width, LANES), half_width)
        return remote(
            part.at[step, :, :, theirs], peer_part.at[shift - 1, step, b],
            swap_send.at[shift - 1, step, b], swap_recv.at[shift - 1, step, b], me, peer,
        )

    def small_route(step, shift):
        return remote(
            route_mine.at[step], peer_route.at[shift - 1, step],
            small_send.at[shift - 1, step], small_recv.at[shift - 1, step],
            me, lax.rem(col + shift, splits),
        )

    def small_square(shift):
        return remote(
            square_mine, peer_square.at[shift - 1], square_send.at[shift - 1], square_recv.at[shift - 1],
            me, lax.rem(col + shift, splits),
        )

    def join_copy(step, b, hop):
        return remote(
            total.at[step, b, hop], gathered.at[step, b, seat],
            join_send.at[step, b, hop], join_recv.at[step, b, hop], group * members + around(hop), col,
        )

    def home_copy(step, b):
        return remote(
            finished.at[step, b], back.at[b, group], home_send.at[step, b], home_recv.at[step, b],
            places[step] * members + seat, col,
        )

    def route_copy(step, hop):
        there = places[step] * members + around(hop)
        return remote(
            route_total.at[step], back_route.at[me], route_send.at[step, hop], route_recv.at[step, hop],
            there, col,
        )

    def pack(step, i):
        cols = window(step, i) if step else pl.ds(i % halves * chunk, chunk)
        source = inputs[i // halves][:, cols]
        return jnp.dot(gsel_ref[places[step]], source, preferred_element_type=f32).astype(bf16)

    def spread(step, i, block):
        choice = landed_choice[step] if step else choice_ref[group]
        value = lax.dot_general(choice, block, (((0,), (0,)), ((), ())), preferred_element_type=f32)
        wide_cut = block.shape[1]
        stage[i, step, :, :, pl.ds(0, wide_cut)] = value.astype(bf16).reshape(members, capacity, wide_cut)
        if step == 0:
            mate_copy(i, mate_out).start()
        each_hop(step, False, True, lambda hop: near_copy(step, hop, i).start())

        cols = window(step, i) if step else pl.ds(i % halves * chunk, chunk)
        rows[i // halves, step, seat, :, cols] = stage[i, step, seat, :, pl.ds(0, wide_cut)]
        if step:
            for shift in relays(step, i):
                relay(step, 0, shift, i, col).start()

    def relays(step, i):
        return () if whole(step, i) else range(1, splits)

    choices = set()

    def arrive(step, i):
        if step not in choices:
            choices.add(step)
            far_copy(step, 2 * halves).wait_recv()
        far_copy(step, i).wait_recv()
        spread(step, i, landed[i, step, :, pl.ds(0, chunk_width(step, i))])

    def forward(step, i):
        def pass_on(hop):
            near_copy(step, hop, i).wait_recv()
            for shift in relays(step, i):
                relay(step, hop, shift, i, col).start()

        each_hop(step, False, False, pass_on)
        if step == 0:
            mate_copy(i, mate_in).wait_recv()

    def complete(step):
        def landed_all(hop):
            for i in chunks:
                for shift in relays(step, i):
                    relay(step, hop, shift, i, lax.rem(col + splits - shift, splits)).wait_recv()

        each_hop(step, True, False, landed_all)

        @pl.loop(0 if step else 1, members)
        def _(hop):
            scale_copy(step, hop).wait_recv()

    def compute(step):
        slot_rows = rows[0, step].reshape(span, model_width)
        slot_cot = rows[1, step].reshape(span, model_width)
        pre = jnp.dot(slot_rows, wide[...], preferred_element_type=f32)
        gate_pre, up_pre = pre[:, :hidden_width], pre[:, hidden_width:]
        hidden_back = lax.dot_general(
            slot_cot, down[...], (((1,), (1,)), ((), ())), preferred_element_type=f32
        )
        spread_scale = jnp.broadcast_to(scale_in[step], (members, capacity, span))
        lane = lax.broadcasted_iota(jnp.int32, (members, capacity, span), 2)
        slot = lax.broadcasted_iota(jnp.int32, (members, capacity, span), 1) + seat * capacity
        scale = jnp.sum(jnp.where(lane == slot, spread_scale, 0.0), axis=2, keepdims=True)
        scale = scale.reshape(span, 1)
        gate_sig = jax.nn.sigmoid(gate_pre)
        activated = gate_pre * gate_sig
        hidden = activated * up_pre
        route = hidden * hidden_back
        folded = route[:, :LANES]
        for start in range(LANES, hidden_width, LANES):
            folded = folded + route[:, start : start + LANES]
        route_mine[step] = jnp.sum(folded.T, axis=0, keepdims=True)
        hidden_cot = scale * hidden_back
        up_cot = (hidden_cot * activated).astype(bf16)
        gate_cot = (hidden_cot * up_pre * gate_sig * (1.0 + gate_pre * (1.0 - gate_sig))).astype(bf16)
        slots = pl.ds(step * span, span)
        cots[slots, pl.ds(0, hidden_width)] = gate_cot
        cots[slots, pl.ds(hidden_width, hidden_width)] = up_cot
        weighted[slots, :] = (scale * hidden).astype(bf16)
        both = cots[slots, :]

        @pl.loop(0, model_width // (2 * TILE))
        def _(tile):
            cols = pl.ds(pl.multiple_of(tile * 2 * TILE, LANES), 2 * TILE)
            term = lax.dot_general(
                both, wide[cols, :], (((1,), (1,)), ((), ())), preferred_element_type=f32
            )
            part[step, :, :, cols] = term.astype(bf16).reshape(members, capacity, 2 * TILE)

        for shift in range(1, splits):
            small_route(step, shift).start()

    def send_swaps(step):
        for b in range(halves):
            for shift in range(1, splits):
                swap(step, b, shift).start()

    def route_home(step):
        value = route_mine[step]
        for shift in range(1, splits):
            small_route(step, shift).wait_recv()
            value = value + peer_route[shift - 1, step]
        route_total[step] = value
        if step == 0:
            back_route[me] = value

        @pl.loop(0 if step else 1, members)
        def _(hop):
            route_copy(step, hop).start()

    def block_total(step, b, hop):
        source = around(hop)
        mine = pl.ds(pl.multiple_of(col * width + b * half_width, LANES), half_width)
        value = part[step, source, :, mine].astype(f32)
        for shift in range(1, splits):
            value = value + peer_part[shift - 1, step, b, source].astype(f32)
        return value.astype(bf16)

    def reduce(step, b):
        for shift in range(1, splits):
            swap(step, b, shift).wait_recv()

        @pl.loop(1, members)
        def _(hop):
            total[step, b, hop] = block_total(step, b, hop)
            join_copy(step, b, hop).start()

        gathered[step, b, seat] = block_total(step, b, 0)

    def collect(step, b):
        @pl.loop(1, members)
        def _(hop):
            join_copy(step, b, hop).wait_recv()

        pairs = gathered[step, b].reshape(span, half_width)
        choice = landed_choice[step] if step else choice_ref[group]
        summed = jnp.dot(choice, pairs, preferred_element_type=f32).astype(bf16)
        if step:
            finished[step, b] = summed
            home_copy(step, b).start()
        else:
            back[b, group] = summed

    def lane_sums(value):
        folded = value[:, :LANES]
        for start in range(LANES, value.shape[1], LANES):
            folded = folded + value[:, start : start + LANES]
        return folded

    def grads_in(first):
        tiles = model_width // TILE // 2

        @pl.loop(first * tiles, (first + 1) * tiles)
        def _(tile):
            cols = pl.ds(pl.multiple_of(tile * TILE, LANES), TILE)
            left = rows[0, :, :, :, cols].reshape(GROUPS * span, TILE)
            grad = lax.dot_general(
                left, cots[...], (((0,), (0,)), ((), ())), preferred_element_type=f32
            ).astype(bf16)
            for n, out in enumerate((gate_out, up_out)):
                value = grad[:, n * hidden_width : (n + 1) * hidden_width]
                out[cols, :] = value
                square = lane_sums(jnp.square(value.astype(f32)))
                square_mine[n, :, cols] = jnp.sum(square.T, axis=0, keepdims=True)

    def grads_down(first):
        tiles = model_width // TILE // 4

        @pl.loop(first * tiles, (first + 1) * tiles)
        def _(tile):
            cols = pl.ds(pl.multiple_of(tile * 2 * TILE, LANES), 2 * TILE)
            right = rows[1, :, :, :, cols].reshape(GROUPS * span, 2 * TILE)
            grad = lax.dot_general(
                weighted[...], right, (((0,), (0,)), ((), ())), preferred_element_type=f32
            ).astype(bf16)
            down_out[:, cols] = grad
            down_acc[...] += lane_sums(jnp.square(grad.astype(f32)))

    for load in route_loads:
        load.wait()
    topk, tok_rows = ids_ref.shape
    group_cap = gsel_ref.shape[1]

    def count(shape, axis):
        return lax.broadcasted_iota(jnp.int32, shape, axis).astype(f32)

    def one_hot(mask):
        return mask.astype(f32).astype(bf16)

    ids = [ids_ref[pl.ds(k, 1), :].astype(f32) for k in range(topk)]
    expert_count = count((experts, tok_rows), 0)
    picks = [(expert_count == value).astype(f32) for value in ids]
    named = sum(picks).astype(bf16)
    earlier = one_hot(count((tok_rows, tok_rows), 0) < count((tok_rows, tok_rows), 1))
    before_it = jnp.dot(named, earlier, preferred_element_type=f32)
    ranks = [jnp.sum(pick * before_it, axis=0, keepdims=True) for pick in picks]
    group_count = count((4 * GROUPS, tok_rows), 0) * members
    in_group = ((ids[0] >= group_count) & (ids[0] < group_count + members)).astype(f32)
    group_before = jnp.dot(in_group.astype(bf16), earlier, preferred_element_type=f32)
    own_rank = jnp.sum(in_group * group_before, axis=0, keepdims=True)
    for g in range(GROUPS):
        inside = (count((group_cap, tok_rows), 0) == own_rank).astype(f32) * in_group[g : g + 1, :]
        gsel_ref[g] = inside.astype(bf16)

    def make_choice(g):
        slot_count = count((span, tok_rows), 0) + g * span
        hits = [one_hot(slot_count == value * capacity + rank) for value, rank in zip(ids, ranks)]
        choice_ref[g] = lax.dot_general(
            gsel_ref[g], sum(hits), (((1,), (1,)), ((), ())), preferred_element_type=f32
        ).astype(bf16)
        scales = sum(
            lax.dot_general(
                jnp.broadcast_to(weight_ref[pl.ds(k, 1), :].astype(f32), (16, tok_rows)).astype(bf16),
                hits[k], (((1,), (1,)), ((), ())), preferred_element_type=f32,
            )
            for k in range(topk)
        )
        scale_ref[g] = scales[:1]

    def route_back():
        table = back_route[...].reshape(experts, span).astype(bf16)
        lane = count((span, tok_rows), 0) - (seat * capacity).astype(f32)
        for k in range(topk):
            found = lax.dot_general(
                table, picks[k].astype(bf16), (((0,), (0,)), ((), ())), preferred_element_type=f32
            )
            chosen = jnp.where(lane == ranks[k], found, 0.0)
            route_out[pl.ds(k, 1), :] = jnp.sum(chosen, axis=0, keepdims=True).astype(bf16)

    down_acc[...] = jnp.zeros_like(down_acc)
    begun = set()
    grad_parts = [0, 0]

    def first_time(name):
        fresh = name not in begun
        begun.add(name)
        return fresh

    def send_scales():
        scale_in[0, seat] = scale_ref[group]
        for step in range(GROUPS):

            @pl.loop(0 if step else 1, members)
            def _(hop):
                scale_copy(step, hop).start()

    def run(token):
        name, step, i = token[:-2], int(token[-2]), int(token[-1])
        if halves < HALVES and name != "comp" and name != "grad":
            if i % HALVES:
                return
            i = i // HALVES
        if name == "far":
            packed[i, step, :, pl.ds(0, chunk_width(step, i))] = pack(step, i)
            if first_time("far"):
                pl.semaphore_wait(barrier, experts - 1 + splits - 1)
            far_copy(step, i).start()
        elif name == "spread":
            if first_time("spread"):
                for g in range(GROUPS):
                    make_choice(g)
                for other in range(1, GROUPS):
                    far_copy(other, 2 * halves).start()
            if step:
                arrive(step, i)
            else:
                spread(step, i, pack(step, i))
        elif name == "fwd":
            if first_time("fwd"):
                send_scales()
            forward(step, i)
        elif name == "comp":
            if first_time("comp"):
                for load in weight_loads:
                    load.wait()
            complete(step)
            compute(step)
            send_swaps(step)
        elif name == "red":
            if first_time("route%d" % step):
                route_home(step)
            reduce(step, i)
        elif name == "col":
            collect(step, i)
        elif step < 2:
            grads_in(grad_parts[0])
            grad_parts[0] += 1
            if grad_parts[0] == 2:
                for shift in range(1, splits):
                    small_square(shift).start()
        else:
            grads_down(grad_parts[1])
            grad_parts[1] += 1
            if grad_parts[1] == 2:
                down_square_out[...] = jnp.sum(down_acc[...].T, axis=0, keepdims=True)

    for load in input_loads:
        load.wait()
    for token in PLAN:
        run(token)

    for step in range(GROUPS):

        @pl.loop(0 if step else 1, members)
        def _(hop):
            route_copy(step, hop).wait_recv()

    route_back()
    for shift in range(1, splits):
        small_square(shift).wait_recv()
    value = square_mine[...]
    for shift in range(1, splits):
        value = value + peer_square[shift - 1]
    gate_square_out[...] = value[0]
    up_square_out[...] = value[1]
    selector = gsel_ref[...].reshape(GROUPS * group_cap, tok_rows)
    for b in range(halves):
        for step in range(1, GROUPS):
            home_copy(step, b).wait_recv()
        token_out[:, pl.ds(b * half_width, half_width)] = lax.dot_general(
            selector, back[b].reshape(GROUPS * group_cap, half_width), (((0,), (0,)), ((), ())),
            preferred_element_type=f32,
        ).astype(bf16)

    for step in range(GROUPS):
        if step:
            for b in range(halves):
                home_copy(step, b).wait_send()
            for i in range(2 * halves + 1):
                far_copy(step, i).wait_send()

        for i in chunks:
            each_hop(step, False, True, lambda hop: near_copy(step, hop, i).wait_send())
            if step == 0:
                mate_copy(i, mate_out).wait_send()

        @pl.loop(1, members)
        def _(hop):
            for b in range(halves):
                join_copy(step, b, hop).wait_send()

        def relays_sent(hop):
            for i in chunks:
                for shift in relays(step, i):
                    relay(step, hop, shift, i, col).wait_send()

        each_hop(step, True, False, relays_sent)

        for shift in range(1, splits):
            for b in range(halves):
                swap(step, b, shift).wait_send()

        @pl.loop(0 if step else 1, members)
        def _(hop):
            scale_copy(step, hop).wait_send()
            route_copy(step, hop).wait_send()

        for shift in range(1, splits):
            small_route(step, shift).wait_send()
    for shift in range(1, splits):
        small_square(shift).wait_send()


def layer(ids, weights, tokens, cot, gate, up, down, experts, splits):
    members = experts // GROUPS
    topk, tok_rows = ids.shape
    model_width = tokens.shape[1]
    capacity = 2 * tok_rows * topk // experts
    span = members * capacity
    group_cap = span // topk
    hidden_width = gate.shape[1]
    width = model_width // splits
    halves = HALVES if experts * splits <= 64 else 1
    half_width, chunk, chunks = width // halves, model_width // halves, 2 * halves
    f32, bf16 = jnp.float32, jnp.bfloat16
    vmem = pl.BlockSpec(memory_space=pltpu.VMEM)
    hbm = pl.BlockSpec(memory_space=pltpu.HBM)
    ids, weights, tokens, cot, gate, up, down = (
        pltpu.with_memory_space_constraint(v, pltpu.HBM)
        for v in (ids, weights, tokens, cot, gate, up, down)
    )
    dma = pltpu.SemaphoreType.DMA
    shape = jax.ShapeDtypeStruct
    slots = (GROUPS, members, capacity)
    return pl.pallas_call(
        functools.partial(layer_kernel, experts, splits),
        out_shape=(
            shape((tok_rows, width), bf16),
            shape((topk, tok_rows), bf16),
            shape((model_width, hidden_width), bf16),
            shape((model_width, hidden_width), bf16),
            shape((1, model_width), f32),
            shape((1, model_width), f32),
            shape((hidden_width, model_width), bf16),
            shape((1, hidden_width), f32),
        ),
        in_specs=[hbm] * 7,
        out_specs=(vmem,) * 8,
        scratch_shapes=[
            pltpu.VMEM((topk, tok_rows), jnp.int32),
            pltpu.VMEM((topk, tok_rows), bf16),
            pltpu.VMEM((tok_rows, model_width), bf16),
            pltpu.VMEM((tok_rows, model_width), bf16),
            pltpu.VMEM((GROUPS, group_cap, tok_rows), bf16),
            pltpu.VMEM((GROUPS, group_cap, span), bf16),
            pltpu.VMEM((GROUPS, 1, span), f32),
            pltpu.VMEM((experts, 1, span), f32),
            pltpu.VMEM((chunks, GROUPS, group_cap, chunk), bf16),
            pltpu.VMEM((chunks, GROUPS, group_cap, chunk), bf16),
            pltpu.VMEM((GROUPS, group_cap, span), bf16),
            pltpu.VMEM((chunks,) + slots + (chunk,), bf16),
            pltpu.VMEM((2,) + slots + (model_width,), bf16),
            pltpu.VMEM((GROUPS, members, 1, span), f32),
            pltpu.VMEM((model_width, 2 * hidden_width), bf16),
            pltpu.VMEM((hidden_width, model_width), bf16),
            pltpu.VMEM((GROUPS * span, 2 * hidden_width), bf16),
            pltpu.VMEM((GROUPS * span, hidden_width), bf16),
            pltpu.VMEM(slots + (model_width,), bf16),
            pltpu.VMEM((splits - 1, GROUPS, halves) + slots[1:] + (half_width,), bf16),
            pltpu.VMEM((GROUPS, halves) + slots[1:] + (half_width,), bf16),
            pltpu.VMEM((GROUPS, halves) + slots[1:] + (half_width,), bf16),
            pltpu.VMEM((GROUPS, halves, group_cap, half_width), bf16),
            pltpu.VMEM((halves, GROUPS, group_cap, half_width), bf16),
            pltpu.VMEM((GROUPS, 1, span), f32),
            pltpu.VMEM((splits - 1, GROUPS, 1, span), f32),
            pltpu.VMEM((GROUPS, 1, span), f32),
            pltpu.VMEM((2, 1, model_width), f32),
            pltpu.VMEM((splits - 1, 2, 1, model_width), f32),
            pltpu.VMEM((hidden_width, LANES), f32),
            dma((chunks + 1, GROUPS)), dma((chunks + 1, GROUPS)),
            dma((chunks, GROUPS, members)), dma((chunks, GROUPS, members)),
            dma((chunks, splits - 1, GROUPS, members)), dma((chunks, splits - 1, GROUPS, members)),
            dma((GROUPS, members)), dma((GROUPS, members)),
            dma((splits - 1, GROUPS, halves)), dma((splits - 1, GROUPS, halves)),
            dma((GROUPS, halves, members)), dma((GROUPS, halves, members)),
            dma((GROUPS, halves)), dma((GROUPS, halves)),
            dma((splits - 1, GROUPS)), dma((splits - 1, GROUPS)),
            dma((GROUPS, members)), dma((GROUPS, members)),
            dma((splits - 1,)), dma((splits - 1,)),
            dma((7,)),
        ],
        compiler_params=pltpu.CompilerParams(
            collective_id=0, has_side_effects=True, vmem_limit_bytes=40000 * 1024
        ),
    )(ids, weights, tokens, cot, gate, up, down)


def export_kernel(*refs):
    count = len(refs) // 2
    copies = [
        pltpu.make_async_copy(refs[n], refs[count + n], refs[-1].at[n]) for n in range(count)
    ]
    for copy in copies:
        copy.start()
    for copy in copies:
        copy.wait()


def export(arrays):
    return pl.pallas_call(
        export_kernel,
        out_shape=tuple(jax.ShapeDtypeStruct(a.shape, a.dtype) for a in arrays),
        in_specs=[pl.BlockSpec(memory_space=pltpu.VMEM)] * len(arrays),
        out_specs=(pl.BlockSpec(memory_space=pltpu.HBM),) * len(arrays),
        scratch_shapes=[pltpu.SemaphoreType.DMA((len(arrays),))],
        compiler_params=pltpu.CompilerParams(vmem_limit_bytes=8000 * 1024),
    )(*arrays)


def on_device(tokens, expert_ids, route_weights, cotangent, w_gate, w_up, w_down):
    experts = lax.axis_size("ep")
    splits = lax.axis_size("tp")
    results = layer(
        expert_ids.T, route_weights.T, tokens, cotangent, w_gate[0], w_up[0], w_down[0], experts, splits
    )
    token_grad, route_grad, grad_gate, grad_up, gate_square, up_square, grad_down, down_square = export(results)
    return (
        token_grad,
        route_grad.T,
        grad_gate[None],
        grad_up[None],
        grad_down[None],
        gate_square,
        up_square,
        down_square,
    )


def solution(mesh):
    return jax.shard_map(
        on_device,
        mesh=mesh,
        in_specs=(
            P("ep", None),
            P("ep", None),
            P("ep", None),
            P("ep", None),
            P("ep", None, "tp"),
            P("ep", None, "tp"),
            P("ep", "tp", None),
        ),
        out_specs=(
            P("ep", "tp"),
            P("ep", None),
            P("ep", None, "tp"),
            P("ep", None, "tp"),
            P("ep", "tp", None),
            P("ep", None),
            P("ep", None),
            P("ep", "tp"),
        ),
        check_vma=False,
    )
```
